32 devices in a mesh: fs: 4 (over y, x), tp: 8 (over z, core).
Axes of the slice: x: 2, y: 2, z: 4, core: 2. Of those that a mesh axis runs over, the one named last changes fastest.
Arguments:
- saved_input: bfloat16 [4096, 4096], P('fs', 'tp'), may hold values from -6 to 6
- query_cot: bfloat16 [4096, 4096], P('fs', 'tp'), may hold values from -6 to 6
- key_cot: bfloat16 [4096, 4096], P('fs', 'tp'), may hold values from -6 to 6
- query_master: float32 [4096, 4096], P('fs', 'tp'), may hold values from -0.09375 to 0.09375
- key_master: float32 [4096, 4096], P('fs', 'tp'), may hold values from -0.09375 to 0.09375
- query_basis: bfloat16 [4096, 256], P('fs'), may hold values from -3 to 3
- key_basis: bfloat16 [4096, 256], P('fs'), may hold values from -3 to 3
- query_first: float32 [256, 4096], P('fs', 'tp'), may hold values from -240 to 240
- query_second: float32 [256, 4096], P('fs', 'tp'), may hold values from 1000 to 20000
- key_first: float32 [256, 4096], P('fs', 'tp'), may hold values from -240 to 240
- key_second: float32 [256, 4096], P('fs', 'tp'), may hold values from 1000 to 20000
Outputs:
- query_step: float32 [4096, 4096], P('fs', 'tp')
- query_weight: float32 [4096, 4096], P('fs', 'tp')
- query_copy: bfloat16 [4096, 4096], P(None, 'tp')
- query_first_new: float32 [256, 4096], P('fs', 'tp')
- query_second_new: float32 [256, 4096], P('fs', 'tp')
- key_step: float32 [4096, 4096], P('fs', 'tp')
- key_weight: float32 [4096, 4096], P('fs', 'tp')
- key_copy: bfloat16 [4096, 4096], P(None, 'tp')
- key_first_new: float32 [256, 4096], P('fs', 'tp')
- key_second_new: float32 [256, 4096], P('fs', 'tp')
The draws below stay inside these ranges and needn't reach their ends.
All inputs are finite; a program needn't handle non-finite values.
Results may differ from the reference program's by a relative error of at most 0.0065.
Values may be sent and summed in bfloat16 or wider, within the bound.
A program may use at most 64 MiB of HBM per device.

```python
import math
import jax
import jax.numpy as jnp
from jax import lax

D = 4096
HEADS = 32
HD = 128
RANK = 256
TOKENS = 4096


def basis_draw(key, salt):
    base = jax.random.fold_in(key, salt)
    entry_key, factor_key = jax.random.split(base)
    group = max(D // 64, 1)
    groups = D // group
    entries = jnp.clip(jax.random.normal(entry_key, (D, RANK), jnp.float32), -4.0, 4.0)
    factors = jnp.exp(jax.random.uniform(factor_key, (groups,), jnp.float32, -1.5, 1.5))
    row_scale = jnp.repeat(factors, group)
    values = entries * row_scale[:, None] * D ** (-0.5)
    return values.astype(jnp.bfloat16)


def draw_query_basis(key, part):
    return basis_draw(key, 101)


def draw_key_basis(key, part):
    return basis_draw(key, 202)


def block_scale(key, dims, pieces, low, largest):
    loudness, own = 1.0, jax.random.fold_in(key, 6)
    for position, blocks in pieces:
        steps = jnp.exp(jax.random.uniform(jax.random.fold_in(own, position), (blocks,), jnp.float32, low / len(pieces), largest / len(pieces)))
        loudness = loudness * jnp.repeat(steps, dims[position] // blocks).reshape([-1 if axis == position else 1 for axis in range(len(dims))])
    return loudness


def bell_draw(stream_key, shape, scale, most, cuts=(), kind=jnp.bfloat16):
    values = jax.random.normal(stream_key, shape, jnp.float32) * scale
    if len(cuts) > 0:
        values = block_scale(stream_key, shape, cuts, -0.22, 0.18) * values
    return jnp.clip(values, min=-most, max=most).astype(kind)


def setup_inputs(seed: int = 0) -> dict:
    seeds = jax.random.split(jax.random.key(seed), 12)
    saved_input = bell_draw(seeds[0], (TOKENS, D), 1.0, 6.0, ((0, 4), (1, 8)))
    query_cot = bell_draw(seeds[1], (TOKENS, HEADS * HD), 1.0, 6.0, ((0, 4), (1, 8)))
    key_cot = bell_draw(seeds[2], (TOKENS, HEADS * HD), 1.0, 6.0, ((0, 4), (1, 8)))
    query_master = bell_draw(seeds[3], (D, HEADS * HD), D ** -0.5, 0.09375, ((0, 4), (1, 8)), jnp.float32)
    key_master = bell_draw(seeds[4], (D, HEADS * HD), D ** -0.5, 0.09375, ((0, 4), (1, 8)), jnp.float32)
    query_basis = draw_query_basis(jax.random.fold_in(seeds[11], 71), 0)
    key_basis = draw_key_basis(jax.random.fold_in(seeds[11], 71), 0)
    query_first = bell_draw(seeds[7], (RANK, HEADS * HD), 40.0, 240.0, ((0, 4), (1, 8)), jnp.float32)
    query_second = jnp.clip(jnp.exp(math.log(20000.0) - 2.9957323 * jax.random.uniform(seeds[8], (RANK, HEADS * HD), jnp.float32) ** block_scale(seeds[8], (RANK, HEADS * HD), ((0, 4), (1, 8)), -0.2, 0.2)), 1000.0, 20000.0)
    key_first = bell_draw(seeds[9], (RANK, HEADS * HD), 40.0, 240.0, ((0, 4), (1, 8)), jnp.float32)
    key_second = jnp.clip(jnp.exp(math.log(20000.0) - 2.9957323 * jax.random.uniform(seeds[10], (RANK, HEADS * HD), jnp.float32) ** block_scale(seeds[10], (RANK, HEADS * HD), ((0, 4), (1, 8)), -0.2, 0.2)), 1000.0, 20000.0)
    return {"saved_input": saved_input, "query_cot": query_cot, "key_cot": key_cot, "query_master": query_master, "key_master": key_master, "query_basis": query_basis, "key_basis": key_basis, "query_first": query_first, "query_second": query_second, "key_first": key_first, "key_second": key_second}


moment_decay = 0.8
square_decay = 0.9
square_floor = 1.0
norm_floor = 0.01
step_rate = 0.01

def update_one(saved_input, cotangent, master, basis, first, second):
    grad = jnp.dot(saved_input.T, cotangent, preferred_element_type=jnp.float32)
    low = jnp.dot(basis.astype(jnp.float32).T, grad, precision=lax.Precision.HIGHEST)
    first_new = moment_decay * first + (1.0 - moment_decay) * low
    second_new = square_decay * second + (1.0 - square_decay) * low * low
    ratio = (first_new / jnp.sqrt(second_new + square_floor)).astype(jnp.bfloat16)
    update = jnp.dot(basis, ratio, preferred_element_type=jnp.float32)
    by_head = update.reshape(D, HEADS, HD)
    head_mean = lax.optimization_barrier(jnp.mean(by_head * by_head, axis=(0, 2)))
    head_scale = 1.0 / jnp.sqrt(head_mean + norm_floor)
    step = (by_head * head_scale[None, :, None]).reshape(D, HEADS * HD)
    weight = master - step_rate * step
    return (step, weight, weight.astype(jnp.bfloat16), first_new, second_new)

def reference(saved_input, query_cot, key_cot, query_master, key_master, query_basis, key_basis, query_first, query_second, key_first, key_second):
    query_out = update_one(saved_input, query_cot, query_master, query_basis, query_first, query_second)
    key_out = update_one(saved_input, key_cot, key_master, key_basis, key_first, key_second)
    return (query_out[0], query_out[1], query_out[2], query_out[3], query_out[4], key_out[0], key_out[1], key_out[2], key_out[3], key_out[4])
```

```python
import functools

import jax
import jax.numpy as jnp
from jax import lax
from jax.experimental import pallas as pl
from jax.experimental.pallas import tpu as pltpu
from jax.sharding import PartitionSpec as P

HD = 128

moment_decay = 0.8
square_decay = 0.9
square_floor = 1.0
norm_floor = 0.01
step_rate = 0.01

BF = jnp.bfloat16
F32 = jnp.float32
MESH = pl.DeviceIdType.MESH


def exchange_kernel(
    fs,
    tp,
    x_hbm,
    qc_hbm,
    kc_hbm,
    qm_hbm,
    km_hbm,
    qb_hbm,
    kb_hbm,
    qf_hbm,
    qs_hbm,
    kf_hbm,
    ks_hbm,
    first_new,
    second_new,
    step_ref,
    weight_ref,
    copy_ref,
    basis,
    gathered,
    x_v,
    cot,
    master,
    moment,
    half_send,
    half_recv,
    half_own,
    z_send,
    z_recv,
    low,
    proj,
    proj_send,
    proj_recv,
    ratio,
    sums,
    scales,
    load_sem,
    b_send,
    b_recv,
    d_send,
    d_recv,
    p_send,
    p_recv,
    zr_send,
    zr_recv,
    zg_send,
    zg_recv,
    pf_send,
    pf_recv,
    g_send,
    g_recv,
    gp_send,
    gp_recv,
    rs_send,
    rs_recv,
    ag_send,
    ag_recv,
    s_send,
    s_recv,
    m_send,
    m_recv,
    r_send,
    r_recv,
):
    f = lax.axis_index("fs")
    t = lax.axis_index("tp")
    z, c = t // 2, t % 2
    depth = tp // 2
    relay = fs == 4
    rows, rank = qb_hbm.shape
    width = qc_hbm.shape[1]
    tokens, columns = x_v.shape
    part = rank // fs
    half = tokens // 2
    chunk = tokens // tp
    group = rows // columns
    owner = t // group
    role = f ^ owner
    tile = min(rows, 128)
    pieces = rows // tile

    def at(start, size):
        return pl.ds(pl.multiple_of(start, size), size)

    def remote(src, dst, send, recv, df, dt):
        return pltpu.make_async_remote_copy(
            src_ref=src,
            dst_ref=dst,
            send_sem=send,
            recv_sem=recv,
            device_id=(df, dt),
            device_id_type=MESH,
        )

    own_rows = at(f * rows, rows)
    sources = (
        (qb_hbm, basis.at[0, own_rows]),
        (kb_hbm, basis.at[1, own_rows]),
        (qm_hbm, master.at[0]),
        (km_hbm, master.at[1]),
        (x_hbm, x_v),
        (qc_hbm, cot.at[0]),
        (kc_hbm, cot.at[1]),
        (qf_hbm, moment.at[0]),
        (qs_hbm, moment.at[1]),
        (kf_hbm, moment.at[2]),
        (ks_hbm, moment.at[3]),
    )
    loads = [
        pltpu.make_async_copy(source, target, load_sem.at[i])
        for i, (source, target) in enumerate(sources)
    ]
    for load in loads:
        load.start()

    barrier = pltpu.get_barrier_semaphore()
    for m in range(1, fs):
        pl.semaphore_signal(barrier, inc=1, device_id=(f ^ m, t), device_id_type=MESH)
    pl.semaphore_signal(barrier, inc=1, device_id=(f, t ^ 1), device_id_type=MESH)
    for d in range(1, depth):
        other = lax.rem(z + d, depth) * 2 + c
        pl.semaphore_signal(barrier, inc=1, device_id=(f, other), device_id_type=MESH)

    def master_copy(m, j, i):
        piece = gathered.at[j, at(f * rows + i * tile, tile)]
        return remote(piece, piece, m_send.at[m - 1], m_recv.at[m - 1, j, i], f ^ m, t)

    def relay_copy(m, i):
        piece = gathered.at[2 - m, at((f ^ (3 - m)) * rows + i * tile, tile)]
        return remote(piece, piece, r_send.at[m - 1], r_recv.at[m - 1, i], f ^ m, t)

    def issue(m, start, stop):
        for turn in range(2):
            j = (m + 1 + turn) % 2
            low_end, high_end = max(start, turn * pieces), min(stop, (turn + 1) * pieces)
            if low_end < high_end:

                @pl.loop(low_end - turn * pieces, high_end - turn * pieces)
                def _(i, j=j):
                    master_copy(m, j, i).start()

        low_end, high_end = max(start, 2 * pieces), min(stop, 3 * pieces)
        if low_end < high_end:

            @pl.loop(low_end - 2 * pieces, high_end - 2 * pieces)
            def _(i):
                master_copy(3 - m, 2 - m, i).wait_recv()
                relay_copy(m, i).start()

    def share(start, stop):
        for m in (1, 2):
            issue(m, start, stop)

    count = 3 * pieces
    marks = [count * k // 24 for k in MARKS]

    piece_rows = columns // 2

    def basis_copy(m, j, h, target):
        piece = basis.at[j, at(t * columns + h * piece_rows, piece_rows)]
        return remote(piece, piece, b_send.at[m, j, h], b_recv.at[j, h], target, t)

    loads[0].wait()
    loads[1].wait()
    pl.semaphore_wait(barrier, fs - 1 + depth)
    if relay:

        @pl.when(role == 0)
        def _():
            for j in range(2):
                basis_copy(0, j, 0, f ^ 1).start()
                basis_copy(0, j, 1, f ^ 2).start()
    else:

        @pl.when(role == 0)
        def _():
            for m in range(1, fs):
                for j in range(2):
                    for h in range(2):
                        basis_copy(m, j, h, f ^ m).start()

    for j in range(2):
        loads[2 + j].wait()

        @pl.loop(0, pieces)
        def _(i, j=j):
            gathered[j, at(f * rows + i * tile, tile), :] = master[j, at(i * tile, tile), :].astype(BF)

    if relay:
        first_marks = [[count * k // 24 for k in pair] for pair in FIRST]

        for k in range(4):

            @pl.when(role == k)
            def _(k=k):
                issue(1, 0, first_marks[k][0])
                issue(2, 0, first_marks[k][1])

        @pl.when(role == 1)
        def _():
            for j in range(2):
                basis_copy(0, j, 0, f ^ 2).wait_recv()
                basis_copy(0, j, 0, f ^ 2).start()

        @pl.when(role == 2)
        def _():
            for j in range(2):
                basis_copy(0, j, 1, f ^ 1).wait_recv()
                basis_copy(0, j, 1, f ^ 1).start()

        @pl.when(role == 3)
        def _():
            for j in range(2):
                basis_copy(0, j, 0, f ^ 1).wait_recv()
                basis_copy(0, j, 0, f ^ 1).start()
                basis_copy(0, j, 1, f ^ 2).wait_recv()
                basis_copy(0, j, 1, f ^ 2).start()

        for k in range(4):

            @pl.when(role == k)
            def _(k=k):
                issue(1, first_marks[k][0], marks[0])
                issue(2, first_marks[k][1], marks[0])
    else:
        for m in range(1, fs):
            for j in range(2):

                @pl.loop(0, pieces)
                def _(i, m=m, j=j):
                    master_copy(m, j, i).start()

    def basis_wait(j):
        if relay:

            @pl.when(role == 1)
            def _():
                basis_copy(0, j, 1, f).wait_recv()

            @pl.when(role == 2)
            def _():
                basis_copy(0, j, 0, f).wait_recv()
        else:

            @pl.when(role != 0)
            def _():
                for h in range(2):
                    basis_copy(0, j, h, f).wait_recv()

    def partner_copy(j):
        piece = basis.at[j, at(t * columns, columns)]
        return remote(piece, piece, d_send.at[j], d_recv.at[j], f, t ^ 1)

    step = min(half, 256)

    def project(start, j):
        return jnp.dot(
            x_v[at(start, step), :],
            basis[j, at(t * columns, columns), :],
            preferred_element_type=F32,
        )

    def swap(j):
        return remote(half_send.at[j], half_recv.at[j], p_send.at[j], p_recv.at[j], f, t ^ 1)

    def z_copy(j, d):
        other = lax.rem(z + d, depth)
        return remote(
            z_send.at[j, at(other * chunk, chunk)],
            z_recv.at[d, j],
            zr_send.at[j, d],
            zr_recv.at[j, d],
            f,
            other * 2 + c,
        )

    loads[4].wait()
    for j in range(2):
        basis_wait(j)

        @pl.loop(0, half // step)
        def _(i, j=j):
            half_send[j, at(i * step, step), :] = project((1 - c) * half + i * step, j).astype(BF)

        swap(j).start()

        @pl.loop(0, half // step)
        def _(i, j=j):
            half_own[j, at(i * step, step), :] = project(c * half + i * step, j)

        @pl.when(role != 0)
        def _(j=j):
            partner_copy(j).start()

        swap(j).wait_recv()

        @pl.loop(0, half // chunk)
        def _(i, j=j):
            place = at(i * chunk, chunk)
            both = half_own[j, place, :] + half_recv[j, place, :].astype(F32)
            half_own[j, place, :] = both
            z_send[j, place, :] = both.astype(BF)

        for d in range(1, depth):
            z_copy(j, d).start()

    def low_piece(j, d, core):
        return low.at[j, at(core * half + lax.rem(z + depth - d, depth) * chunk, chunk)]

    def g_copy(j, d):
        other = lax.rem(z + d, depth)
        return remote(
            low_piece(j, 0, c),
            low_piece(j, 0, c),
            zg_send.at[j, d],
            zg_recv.at[j, d],
            f,
            other * 2 + c,
        )

    def forward(j, d):
        return remote(
            low_piece(j, d, c), low_piece(j, d, c), pf_send.at[j, d], pf_recv.at[j, d], f, t ^ 1
        )

    for j in range(2):
        total = half_own[j, at(z * chunk, chunk), :]
        for d in range(1, depth):
            z_copy(j, d).wait_recv()
            total = total + z_recv[d, j].astype(F32)
        low[j, at(c * half + z * chunk, chunk), :] = total.astype(BF)
        for d in range(1, depth):
            g_copy(j, d).start()
        forward(j, 0).start()

    def block_copy(j, o, side, target):
        piece = basis.at[j, at((2 * o + c) * columns, columns)]
        return remote(
            piece, piece, g_send.at[side, o, j], g_recv.at[o, j], f, target * 2 + c
        )

    def block_forward(j, o):
        piece = basis.at[j, at((2 * o + c) * columns, columns)]
        return remote(piece, piece, gp_send.at[o, j], gp_recv.at[o, j], f, t ^ 1)

    def needed(o):
        return f != (2 * o) // group

    def spread(j, o, side):
        if side == 0:

            @pl.when(z >= 1)
            def _():
                block_copy(j, o, 0, z - 1).start()
        else:

            @pl.when(z <= depth - 2)
            def _():
                block_copy(j, o, 1, z + 1).start()

    @pl.when(needed(z))
    def _():
        for j in range(2):
            for side in range(2):
                spread(j, z, side)

    def arrive(s):
        for side in range(2):
            o = z + s if side == 0 else z - s
            inside = o <= depth - 1 if side == 0 else o >= 0

            @pl.when(inside & needed(o))
            def _(o=o, side=side):
                for j in range(2):
                    block_copy(j, o, side, z).wait_recv()
                    spread(j, o, side)
                    block_forward(j, o).start()

    loads[5].wait()
    loads[6].wait()

    def reduce_copy(m, j):
        return remote(
            proj_send.at[j, at((f ^ m) * part, part)],
            proj_recv.at[m, j],
            rs_send.at[m, j],
            rs_recv.at[m, j],
            f ^ m,
            t,
        )

    for j in range(2):
        for d in range(1, depth):
            g_copy(j, d).wait_recv()
            forward(j, d).start()
        for d in range(depth):
            forward(j, d).wait_recv()
        product = lax.dot_general(
            low[j], cot[j], (((0,), (0,)), ((), ())), preferred_element_type=F32
        )
        proj[j] = product
        proj_send[j] = product.astype(BF)
        for m in range(1, fs):
            reduce_copy(m, j).start()
        if relay:
            share(marks[j], marks[j + 1])

    for i in range(7, 11):
        loads[i].wait()
    own = at(f * part, part)

    def ratio_copy(m, j):
        piece = ratio.at[j, own]
        return remote(piece, piece, ag_send.at[m, j], ag_recv.at[m, j], f ^ m, t)

    for j in range(2):
        for m in range(1, fs):
            reduce_copy(m, j).wait_recv()
        summed = proj[j, own, :]
        for m in range(1, fs):
            summed = summed + proj_recv[m, j].astype(F32)
        first = moment_decay * moment[2 * j] + (1.0 - moment_decay) * summed
        second = square_decay * moment[2 * j + 1] + (1.0 - square_decay) * summed * summed
        first_new[j] = first
        second_new[j] = second
        ratio[j, own, :] = (first / jnp.sqrt(second + square_floor)).astype(BF)
        for m in range(1, fs):
            ratio_copy(m, j).start()
        if relay:
            share(marks[j + 2], marks[j + 3])

    arrive(1)

    high = min(rows, 256)
    for j in range(2):
        for m in range(1, fs):
            ratio_copy(m, j).wait_recv()

        def add(i, total, j=j):
            update = jnp.dot(
                basis[j, at(f * rows + i * high, high), :], ratio[j], preferred_element_type=F32
            )
            step_ref[j, at(i * high, high), :] = update
            return total + jnp.sum((update * update).reshape(high // 8, 8, width), axis=0)

        sums[f, j] = lax.fori_loop(0, rows // high, add, jnp.zeros((8, width), F32))

    def sums_copy(m):
        return remote(sums.at[f], sums.at[f], s_send.at[m], s_recv.at[m], f ^ m, t)

    for m in range(1, fs):
        sums_copy(m).start()
    if relay:
        share(marks[4], count)
    for s in range(2, depth):
        arrive(s)
    for m in range(1, fs):
        sums_copy(m).wait_recv()
    for j in range(2):
        squares = sums[0, j]
        for k in range(1, fs):
            squares = squares + sums[k, j]
        squares = jnp.sum(squares, axis=0, keepdims=True)
        for h in range(width // HD):
            head = slice(h * HD, (h + 1) * HD)
            total = jnp.sum(squares[:, head], axis=1, keepdims=True)
            scale = 1.0 / jnp.sqrt(total / (fs * rows * HD) + norm_floor)
            scales[j, :, head] = jnp.broadcast_to(scale, (8, HD))

    def finish(j, place, update):
        step = update * scales[j, 0:1, :]
        copy_ref[j, place, :] = (gathered[j, place, :].astype(F32) - step_rate * step).astype(BF)
        return step

    for j in range(2):

        @pl.loop(0, rows // high)
        def _(i, j=j):
            place = at(i * high, high)
            step = finish(j, at(f * rows + i * high, high), step_ref[j, place, :])
            step_ref[j, place, :] = step
            weight_ref[j, place, :] = master[j, place, :] - step_rate * step

    for j in range(2):

        @pl.when(role != 0)
        def _(j=j):
            partner_copy(j).wait_recv()

    for s in range(1, depth):
        for o, inside in ((z + s, z + s <= depth - 1), (z - s, z - s >= 0)):

            @pl.when(inside & needed(o))
            def _(o=o):
                for j in range(2):
                    block_forward(j, o).wait_recv()

    def finish_rows(j, start):
        place = at(start, high)
        update = jnp.dot(basis[j, place, :], ratio[j], preferred_element_type=F32)
        finish(j, place, update)

    span = high // tile

    def finish_block(m, j, wait):
        @pl.loop(0, rows // high)
        def _(i):
            if wait is not None:
                for k in range(span):
                    wait(i * span + k)
            finish_rows(j, (f ^ m) * rows + i * high)

    if relay:
        finish_block(1, 0, None)
        finish_block(2, 1, None)
        finish_block(1, 1, lambda i: master_copy(1, 1, i).wait_recv())
        finish_block(2, 0, lambda i: master_copy(2, 0, i).wait_recv())

        @pl.loop(0, rows // high)
        def _(i):
            for m in (2, 1):
                for k in range(span):
                    relay_copy(m, i * span + k).wait_recv()
                finish_rows(2 - m, (f ^ 3) * rows + i * high)
    else:
        for m in range(1, fs):
            for j in range(2):
                finish_block(m, j, lambda i, m=m, j=j: master_copy(m, j, i).wait_recv())

    if relay:

        @pl.when(role != 2)
        def _():
            for j in range(2):
                basis_copy(0, j, 0, f).wait_send()

        @pl.when(role != 1)
        def _():
            for j in range(2):
                basis_copy(0, j, 1, f).wait_send()
    else:

        @pl.when(role == 0)
        def _():
            for m in range(1, fs):
                for j in range(2):
                    for h in range(2):
                        basis_copy(m, j, h, f ^ m).wait_send()

    for j in range(2):

        @pl.when(role != 0)
        def _(j=j):
            partner_copy(j).wait_send()

        swap(j).wait_send()
        for d in range(1, depth):
            z_copy(j, d).wait_send()
            g_copy(j, d).wait_send()
        for d in range(depth):
            forward(j, d).wait_send()
        for m in range(1, fs):
            reduce_copy(m, j).wait_send()
            ratio_copy(m, j).wait_send()
    for m in range(1, fs):
        sums_copy(m).wait_send()

    for s in range(depth):
        for side in range(2):
            o = z + s if side == 0 else z - s
            inside = (o <= depth - 1) & (z >= 1) if side == 0 else (o >= 0) & (z <= depth - 2)

            @pl.when(inside & needed(o))
            def _(o=o, side=side):
                for j in range(2):
                    block_copy(j, o, side, z).wait_send()

            if s > 0:
                there = o <= depth - 1 if side == 0 else o >= 0

                @pl.when(there & needed(o))
                def _(o=o):
                    for j in range(2):
                        block_forward(j, o).wait_send()

    for m in (1, 2) if relay else range(1, fs):
        piece = gathered.at[:, own_rows]
        remote(piece, piece, m_send.at[m - 1], m_recv.at[m - 1, 0, 0], f ^ m, t).wait_send()
    if relay:
        for m in (1, 2):
            piece = gathered.at[2 - m, own_rows]
            remote(piece, piece, r_send.at[m - 1], r_recv.at[m - 1, 0], f ^ m, t).wait_send()


MARKS = (13, 14, 15, 16, 18)
FIRST = ((8, 8), (4, 1), (1, 4), (3, 3))


def final_kernel(*refs):
    first, second, step, weight, copy = refs[:5]
    outs, sem = refs[5:15], refs[15]
    moves = []
    for j in range(2):
        for k, source in enumerate((step, weight, copy, first, second)):
            moves.append((source.at[j], outs[5 * j + k]))
    moves = [pltpu.make_async_copy(a, b, sem.at[i]) for i, (a, b) in enumerate(moves)]
    for move in moves:
        move.start()
    for move in moves:
        move.wait()


def body(fs, tp, *args):
    saved_input, query_cot, _, query_master, key_master, query_basis, key_basis = args[:7]
    rows, rank = query_basis.shape
    tokens, columns = saved_input.shape
    width = query_cot.shape[1]
    part = rank // fs
    depth = tp // 2
    count = fs * rows
    half, chunk = tokens // 2, tokens // tp
    pieces = rows // min(rows, 128)
    hbm = pl.BlockSpec(memory_space=pltpu.HBM)
    vmem = pl.BlockSpec(memory_space=pltpu.VMEM)
    dma = pltpu.SemaphoreType.DMA
    own = pltpu.VMEM((2, rows, width), F32)
    moment = pltpu.VMEM((2, part, width), F32)
    pairs = [dma((fs, 2, 2)), dma((2, 2))]
    for shape in (
        (2,),
        (2,),
        (2, depth),
        (2, depth),
        (2, depth),
    ):
        pairs += [dma(shape), dma(shape)]
    pairs += [dma((2, depth, 2)), dma((depth, 2))]
    for shape in ((depth, 2), (fs, 2), (fs, 2), (fs,)):
        pairs += [dma(shape), dma(shape)]
    links = 2 if fs == 4 else fs - 1
    pairs += [dma((links,)), dma((links, 2, pieces)), dma((2,)), dma((2, pieces))]
    results = pl.pallas_call(
        functools.partial(exchange_kernel, fs, tp),
        name="exchange",
        out_shape=(moment, moment, own, own, pltpu.VMEM((2, count, width), BF)),
        in_specs=[hbm] * 11,
        out_specs=(vmem,) * 5,
        scratch_shapes=[
            pltpu.VMEM((2, count, rank), BF),
            pltpu.VMEM((2, count, width), BF),
            pltpu.VMEM((tokens, columns), BF),
            pltpu.VMEM((2, tokens, width), BF),
            pltpu.VMEM((2, rows, width), F32),
            pltpu.VMEM((4, part, width), F32),
            pltpu.VMEM((2, half, rank), BF),
            pltpu.VMEM((2, half, rank), BF),
            pltpu.VMEM((2, half, rank), F32),
            pltpu.VMEM((2, half, rank), BF),
            pltpu.VMEM((depth, 2, chunk, rank), BF),
            pltpu.VMEM((2, tokens, rank), BF),
            pltpu.VMEM((2, rank, width), F32),
            pltpu.VMEM((2, rank, width), BF),
            pltpu.VMEM((fs, 2, part, width), BF),
            pltpu.VMEM((2, rank, width), BF),
            pltpu.VMEM((fs, 2, 8, width), F32),
            pltpu.VMEM((2, 8, width), F32),
            dma((11,)),
            *pairs,
        ],
        compiler_params=pltpu.CompilerParams(
            collective_id=0, has_side_effects=True, vmem_limit_bytes=40 * 1024 * 1024
        ),
    )(*[pltpu.with_memory_space_constraint(a, pltpu.HBM) for a in args])

    big = jax.ShapeDtypeStruct((rows, width), F32)
    copied = jax.ShapeDtypeStruct((count, width), BF)
    small = jax.ShapeDtypeStruct((part, width), F32)
    return pl.pallas_call(
        final_kernel,
        name="final",
        out_shape=(big, big, copied, small, small) * 2,
        in_specs=[vmem] * 5,
        out_specs=(hbm,) * 10,
        scratch_shapes=[dma((10,))],
        compiler_params=pltpu.CompilerParams(vmem_limit_bytes=20 * 1024 * 1024),
    )(*results)


def solution(mesh):
    split, tall, wide = P("fs", "tp"), P("fs", None), P(None, "tp")
    outs = (split, split, wide, split, split)
    return jax.shard_map(
        functools.partial(body, mesh.shape["fs"], mesh.shape["tp"]),
        mesh=mesh,
        in_specs=(split,) * 5 + (tall, tall) + (split,) * 4,
        out_specs=outs + outs,
        check_vma=False,
    )
```

```python
import functools

import jax
import jax.numpy as jnp
from jax import lax
from jax.experimental import pallas as pl
from jax.experimental.pallas import tpu as pltpu
from jax.sharding import PartitionSpec as P

HD = 128

moment_decay = 0.8
square_decay = 0.9
square_floor = 1.0
norm_floor = 0.01
step_rate = 0.01

BF = jnp.bfloat16
F32 = jnp.float32
MESH = pl.DeviceIdType.MESH


def exchange_kernel(
    fs,
    tp,
    x_hbm,
    qc_hbm,
    kc_hbm,
    qm_hbm,
    km_hbm,
    qb_hbm,
    kb_hbm,
    qf_hbm,
    qs_hbm,
    kf_hbm,
    ks_hbm,
    first_new,
    second_new,
    step_ref,
    weight_ref,
    copy_ref,
    basis,
    gathered,
    x_v,
    cot,
    master,
    moment,
    half_send,
    half_recv,
    half_own,
    z_send,
    z_recv,
    low,
    proj,
    proj_send,
    proj_recv,
    proj_mid,
    ratio,
    sums,
    scales,
    load_sem,
    b_send,
    b_recv,
    d_send,
    d_recv,
    p_send,
    p_recv,
    zr_send,
    zr_recv,
    zg_send,
    zg_recv,
    pf_send,
    pf_recv,
    g_send,
    g_recv,
    gp_send,
    gp_recv,
    rs_send,
    rs_recv,
    ag_send,
    ag_recv,
    s_send,
    s_recv,
    m_send,
    m_recv,
    r_send,
    r_recv,
):
    f = lax.axis_index("fs")
    t = lax.axis_index("tp")
    z, c = t // 2, t % 2
    depth = tp // 2
    relay = fs == 4
    rows, rank = qb_hbm.shape
    width = qc_hbm.shape[1]
    tokens, columns = x_v.shape
    part = rank // fs
    half = tokens // 2
    chunk = tokens // tp
    group = rows // columns
    owner = t // group
    role = f ^ owner
    tile = min(rows, 128)
    pieces = rows // tile

    def at(start, size):
        return pl.ds(pl.multiple_of(start, size), size)

    def remote(src, dst, send, recv, df, dt):
        return pltpu.make_async_remote_copy(
            src_ref=src,
            dst_ref=dst,
            send_sem=send,
            recv_sem=recv,
            device_id=(df, dt),
            device_id_type=MESH,
        )

    own_rows = at(f * rows, rows)
    sources = (
        (qb_hbm, basis.at[0, own_rows]),
        (kb_hbm, basis.at[1, own_rows]),
        (qm_hbm, master.at[0]),
        (km_hbm, master.at[1]),
        (x_hbm, x_v),
        (qc_hbm, cot.at[0]),
        (kc_hbm, cot.at[1]),
        (qf_hbm, moment.at[0]),
        (qs_hbm, moment.at[1]),
        (kf_hbm, moment.at[2]),
        (ks_hbm, moment.at[3]),
    )
    loads = [
        pltpu.make_async_copy(source, target, load_sem.at[i])
        for i, (source, target) in enumerate(sources)
    ]
    for load in loads:
        load.start()

    barrier = pltpu.get_barrier_semaphore()
    for m in range(1, fs):
        pl.semaphore_signal(barrier, inc=1, device_id=(f ^ m, t), device_id_type=MESH)
    pl.semaphore_signal(barrier, inc=1, device_id=(f, t ^ 1), device_id_type=MESH)
    for d in range(1, depth):
        other = lax.rem(z + d, depth) * 2 + c
        pl.semaphore_signal(barrier, inc=1, device_id=(f, other), device_id_type=MESH)

    def master_copy(m, j, i):
        piece = gathered.at[j, at(f * rows + i * tile, tile)]
        return remote(piece, piece, m_send.at[m - 1], m_recv.at[m - 1, j, i], f ^ m, t)

    def relay_copy(m, i):
        piece = gathered.at[2 - m, at((f ^ (3 - m)) * rows + i * tile, tile)]
        return remote(piece, piece, r_send.at[m - 1], r_recv.at[m - 1, i], f ^ m, t)

    def issue(m, start, stop):
        for turn in range(2):
            j = (m + 1 + turn) % 2
            low_end, high_end = max(start, turn * pieces), min(stop, (turn + 1) * pieces)
            if low_end < high_end:

                @pl.loop(low_end - turn * pieces, high_end - turn * pieces)
                def _(i, j=j):
                    master_copy(m, j, i).start()

        low_end, high_end = max(start, 2 * pieces), min(stop, 3 * pieces)
        if low_end < high_end:

            @pl.loop(low_end - 2 * pieces, high_end - 2 * pieces)
            def _(i):
                master_copy(3 - m, 2 - m, i).wait_recv()
                relay_copy(m, i).start()

    def share(start, stop):
        for m in (1, 2):
            issue(m, start, stop)

    count = 3 * pieces
    marks = [count * k // 24 for k in MARKS]

    piece_rows = columns // 2

    def basis_copy(m, j, h, target):
        piece = basis.at[j, at(t * columns + h * piece_rows, piece_rows)]
        return remote(piece, piece, b_send.at[0], b_recv.at[j, h], target, t)

    loads[0].wait()
    loads[1].wait()
    pl.semaphore_wait(barrier, fs - 1 + depth)
    if relay:

        @pl.when(role == 0)
        def _():
            for j in range(2):
                basis_copy(0, j, 0, f ^ 1).start()
                basis_copy(0, j, 1, f ^ 2).start()
    else:

        @pl.when(role == 0)
        def _():
            for m in range(1, fs):
                for j in range(2):
                    for h in range(2):
                        basis_copy(m, j, h, f ^ m).start()

    for j in range(2):
        loads[2 + j].wait()

        @pl.loop(0, pieces)
        def _(i, j=j):
            gathered[j, at(f * rows + i * tile, tile), :] = master[j, at(i * tile, tile), :].astype(BF)

    if relay:
        first_marks = [[count * k // 24 for k in pair] for pair in FIRST]

        for k in range(4):

            @pl.when(role == k)
            def _(k=k):
                issue(1, 0, first_marks[k][0])
                issue(2, 0, first_marks[k][1])

        @pl.when(role == 1)
        def _():
            for j in range(2):
                basis_copy(0, j, 0, f ^ 2).wait_recv()
                basis_copy(0, j, 0, f ^ 2).start()

        @pl.when(role == 2)
        def _():
            for j in range(2):
                basis_copy(0, j, 1, f ^ 1).wait_recv()
                basis_copy(0, j, 1, f ^ 1).start()

        @pl.when(role == 3)
        def _():
            for j in range(2):
                basis_copy(0, j, 0, f ^ 1).wait_recv()
                basis_copy(0, j, 0, f ^ 1).start()
                basis_copy(0, j, 1, f ^ 2).wait_recv()
                basis_copy(0, j, 1, f ^ 2).start()

        for k in range(4):

            @pl.when(role == k)
            def _(k=k):
                issue(1, first_marks[k][0], marks[0])
                issue(2, first_marks[k][1], marks[0])
    else:
        for m in range(1, fs):
            for j in range(2):

                @pl.loop(0, pieces)
                def _(i, m=m, j=j):
                    master_copy(m, j, i).start()

    def basis_wait(j):
        if relay:

            @pl.when(role == 1)
            def _():
                basis_copy(0, j, 1, f).wait_recv()

            @pl.when(role == 2)
            def _():
                basis_copy(0, j, 0, f).wait_recv()
        else:

            @pl.when(role != 0)
            def _():
                for h in range(2):
                    basis_copy(0, j, h, f).wait_recv()

    def partner_copy(j):
        piece = basis.at[j, at(t * columns, columns)]
        return remote(piece, piece, d_send.at[0], d_recv.at[0], f, t ^ 1)

    step = min(half, 256)

    def project(start, j):
        return jnp.dot(
            x_v[at(start, step), :],
            basis[j, at(t * columns, columns), :],
            preferred_element_type=F32,
        )

    def swap(j):
        return remote(half_send.at[j], half_recv.at[j], p_send.at[0], p_recv.at[j], f, t ^ 1)

    def z_copy(j, d):
        other = lax.rem(z + d, depth)
        return remote(
            z_send.at[j, at(other * chunk, chunk)],
            z_recv.at[j, d],
            zr_send.at[0],
            zr_recv.at[j],
            f,
            other * 2 + c,
        )

    loads[4].wait()
    for j in range(2):
        basis_wait(j)

        @pl.loop(0, half // step)
        def _(i, j=j):
            half_send[j, at(i * step, step), :] = project((1 - c) * half + i * step, j).astype(BF)

        swap(j).start()

        @pl.loop(0, half // step)
        def _(i, j=j):
            half_own[j, at(i * step, step), :] = project(c * half + i * step, j)

        @pl.when(role != 0)
        def _(j=j):
            partner_copy(j).start()

        swap(j).wait_recv()

        @pl.loop(0, half // chunk)
        def _(i, j=j):
            place = at(i * chunk, chunk)
            both = half_own[j, place, :] + half_recv[j, place, :].astype(F32)
            half_own[j, place, :] = both
            z_send[j, place, :] = both.astype(BF)

        for d in range(1, depth):
            z_copy(j, d).start()

    def low_piece(j, d, core):
        return low.at[j, at(core * half + lax.rem(z + depth - d, depth) * chunk, chunk)]

    def g_copy(j, d):
        other = lax.rem(z + d, depth)
        return remote(
            low_piece(j, 0, c),
            low_piece(j, 0, c),
            zg_send.at[0],
            zg_recv.at[j, d - 1],
            f,
            other * 2 + c,
        )

    def forward(j, d):
        return remote(
            low_piece(j, d, c), low_piece(j, d, c), pf_send.at[0], pf_recv.at[j], f, t ^ 1
        )

    for j in range(2):
        total = half_own[j, at(z * chunk, chunk), :]
        received = z_recv.at[j, 1:depth]
        remote(received, received, zr_send.at[0], zr_recv.at[j], f, t ^ 1).wait_recv()
        for d in range(1, depth):
            total = total + z_recv[j, d].astype(F32)
        low[j, at(c * half + z * chunk, chunk), :] = total.astype(BF)
        for d in range(1, depth):
            g_copy(j, d).start()
        forward(j, 0).start()

    def block_copy(j, o, side, target):
        piece = basis.at[j, at((2 * o + c) * columns, columns)]
        return remote(
            piece, piece, g_send.at[side, o], g_recv.at[o, j], f, target * 2 + c
        )

    def block_forward(j, o):
        piece = basis.at[j, at((2 * o + c) * columns, columns)]
        return remote(piece, piece, gp_send.at[o], gp_recv.at[o], f, t ^ 1)

    def needed(o):
        return f != (2 * o) // group

    def spread(j, o, side):
        if side == 0:

            @pl.when(z >= 1)
            def _():
                block_copy(j, o, 0, z - 1).start()
        else:

            @pl.when(z <= depth - 2)
            def _():
                block_copy(j, o, 1, z + 1).start()

    @pl.when(needed(z))
    def _():
        for j in range(2):
            for side in range(2):
                spread(j, z, side)

    def arrive(s):
        for side in range(2):
            o = z + s if side == 0 else z - s
            inside = o <= depth - 1 if side == 0 else o >= 0

            @pl.when(inside & needed(o))
            def _(o=o, side=side):
                for j in range(2):
                    block_copy(j, o, side, z).wait_recv()
                    spread(j, o, side)
                    block_forward(j, o).start()

    loads[5].wait()
    loads[6].wait()

    own = at(f * part, part)

    def project_low(j):
        for d in range(1, depth):
            g_copy(j, d).wait_recv()
            forward(j, d).start()
        received = low.at[j, at((1 - c) * half, half)]
        remote(received, received, pf_send.at[0], pf_recv.at[j], f, t ^ 1).wait_recv()
        product = lax.dot_general(
            low[j], cot[j], (((0,), (0,)), ((), ())), preferred_element_type=F32
        )
        proj[j] = product
        proj_send[j] = product.astype(BF)

    def update_moments(j, summed):
        first = moment_decay * moment[2 * j] + (1.0 - moment_decay) * summed
        second = square_decay * moment[2 * j + 1] + (1.0 - square_decay) * summed * summed
        first_new[j] = first
        second_new[j] = second
        ratio[j, own, :] = (first / jnp.sqrt(second + square_floor)).astype(BF)

    def reduce_copy(j, k):
        near, far = (1, 2) if j == 0 else (2, 1)
        if relay:
            source = proj_mid.at[j] if k == 3 else proj_send.at[j, at((f ^ (near, 3)[k - 1]) * part, part)]
            target = f ^ (far if k == 3 else near)
        else:
            source, target = proj_send.at[j, at((f ^ k) * part, part)], f ^ k
        return remote(
            source, proj_recv.at[j, k], rs_send.at[0], rs_recv.at[j, k - 1], target, t
        )

    def ratio_copy(j, k):
        near, far = (1, 2) if j == 0 else (2, 1)
        if relay:
            piece = ratio.at[j, at((f ^ near) * part, part) if k == 3 else own]
            target = f ^ (near if k == 1 else far)
        else:
            piece, target = ratio.at[j, own], f ^ k
        return remote(piece, piece, ag_send.at[0], ag_recv.at[j, k - 1], target, t)

    for j in range(2):
        project_low(j)
        for k in (2, 1) if relay else range(1, fs):
            reduce_copy(j, k).start()
        if relay:
            share(marks[j], marks[j + 1])

    if relay:
        for j in range(2):
            far = 2 if j == 0 else 1
            reduce_copy(j, 2).wait_recv()
            mid = proj[j, at((f ^ far) * part, part), :] + proj_recv[j, 2].astype(F32)
            proj_mid[j] = mid.astype(BF)
            reduce_copy(j, 3).start()
        share(marks[2], marks[3])
    arrive(1)
    for i in range(7, 11):
        loads[i].wait()

    for j in range(2):
        summed = proj[j, own, :]
        for k in (1, 3) if relay else range(1, fs):
            reduce_copy(j, k).wait_recv()
            summed = summed + proj_recv[j, k].astype(F32)
        update_moments(j, summed)
        for k in (1, 2) if relay else range(1, fs):
            ratio_copy(j, k).start()
    if relay:
        share(marks[3], marks[4])
        for j in range(2):
            ratio_copy(j, 1).wait_recv()
            ratio_copy(j, 3).start()
        share(marks[4], marks[5])

    def ratio_wait(j):
        for k in (2, 3) if relay else range(1, fs):
            ratio_copy(j, k).wait_recv()

    if depth > 2:
        arrive(2)

    high = min(rows, 256)
    heads = width // HD
    sums[f] = jnp.zeros(sums.shape[1:], F32)
    for j in range(2):
        ratio_wait(j)

        def add(i, total, j=j):
            update = jnp.dot(
                basis[j, at(f * rows + i * high, high), :], ratio[j], preferred_element_type=F32
            )
            step_ref[j, at(i * high, high), :] = update
            return total + jnp.sum((update * update).reshape(high // 8, 8, width), axis=0)

        squares = lax.fori_loop(0, rows // high, add, jnp.zeros((8, width), F32))
        for h in range(heads):
            total = jnp.sum(squares[:, h * HD : (h + 1) * HD])
            sums[f, j * heads + h : j * heads + h + 1, :] = jnp.broadcast_to(total, (1, HD))

    def sums_copy(m):
        return remote(sums.at[f], sums.at[f], s_send.at[0], s_recv.at[0], f ^ m, t)

    for m in range(1, fs):
        sums_copy(m).start()
    if relay:
        share(marks[5], count)
    for s in range(3, depth):
        arrive(s)
    others = sums.at[0 : fs - 1]
    remote(others, others, s_send.at[0], s_recv.at[0], f ^ 1, t).wait_recv()
    total = sums[0]
    for k in range(1, fs):
        total = total + sums[k]
    factor = 1.0 / jnp.sqrt(total / (fs * rows * HD) + norm_floor)
    for j in range(2):
        for h in range(heads):
            row = factor[j * heads + h : j * heads + h + 1, :]
            scales[j, :, h * HD : (h + 1) * HD] = jnp.broadcast_to(row, (8, HD))

    def finish(j, place, update):
        change = update * (step_rate * scales[j, 0:1, :])
        copy_ref[j, place, :] = (gathered[j, place, :].astype(F32) - change).astype(BF)

    for j in range(2):

        @pl.loop(0, rows // high)
        def _(i, j=j):
            place = at(i * high, high)
            update = step_ref[j, place, :]
            finish(j, at(f * rows + i * high, high), update)
            step = update * scales[j, 0:1, :]
            step_ref[j, place, :] = step
            weight_ref[j, place, :] = master[j, place, :] - step_rate * step

    def both(o, core):
        return basis.at[:, at((2 * o + core) * columns, columns)]

    def partner_block():
        piece = both(z, 1 - c)
        return remote(piece, piece, d_send.at[0], d_recv.at[0], f, t ^ 1)

    @pl.when(role != 0)
    def _():
        partner_block().wait_recv()

    for s in range(1, depth):
        for o, inside in ((z + s, z + s <= depth - 1), (z - s, z - s >= 0)):

            @pl.when(inside & needed(o))
            def _(o=o):
                piece = both(o, 1 - c)
                remote(piece, piece, gp_send.at[o], gp_recv.at[o], f, t ^ 1).wait_recv()

    def finish_rows(j, start):
        place = at(start, high)
        update = jnp.dot(basis[j, place, :], ratio[j], preferred_element_type=F32)
        finish(j, place, update)

    span = high // tile

    def finish_block(m, j, wait):
        @pl.loop(0, rows // high)
        def _(i):
            if wait is not None:
                for k in range(span):
                    wait(i * span + k)
            finish_rows(j, (f ^ m) * rows + i * high)

    if relay:
        finish_block(1, 0, None)
        finish_block(2, 1, None)
        finish_block(1, 1, lambda i: master_copy(1, 1, i).wait_recv())
        finish_block(2, 0, lambda i: master_copy(2, 0, i).wait_recv())

        @pl.loop(0, rows // high)
        def _(i):
            for m in (2, 1):
                for k in range(span):
                    relay_copy(m, i * span + k).wait_recv()
                finish_rows(2 - m, (f ^ 3) * rows + i * high)
    else:
        for m in range(1, fs):
            for j in range(2):
                finish_block(m, j, lambda i, m=m, j=j: master_copy(m, j, i).wait_recv())

    def sent(piece, sem):
        remote(piece, piece, sem, p_recv.at[0], f, t ^ 1).wait_send()

    if relay:
        for k in range(4):

            @pl.when(role == k)
            def _(k=k):
                sent(basis.at[:, 0 : columns if k in (0, 3) else piece_rows], b_send.at[0])
    else:

        @pl.when(role == 0)
        def _():
            for m in range(1, fs):
                sent(basis.at[:, 0:columns], b_send.at[0])

    @pl.when(role != 0)
    def _():
        sent(both(z, c), d_send.at[0])

    sent(half_send, p_send.at[0])
    sent(z_send.at[:, 0 : (depth - 1) * chunk], zr_send.at[0])
    sent(low.at[:, 0 : (depth - 1) * chunk], zg_send.at[0])
    sent(low.at[:, 0 : depth * chunk], pf_send.at[0])
    sent(proj_send.at[:, 0 : (fs - 1) * part], rs_send.at[0])
    sent(ratio.at[:, 0 : (fs - 1) * part], ag_send.at[0])
    sent(others, s_send.at[0])

    for s in range(depth):
        for side in range(2):
            o = z + s if side == 0 else z - s
            there = o <= depth - 1 if side == 0 else o >= 0
            inside = there & (z >= 1) if side == 0 else there & (z <= depth - 2)

            @pl.when(inside & needed(o))
            def _(o=o, side=side):
                sent(both(o, c), g_send.at[side, o])

            if s > 0:

                @pl.when(there & needed(o))
                def _(o=o):
                    sent(both(o, c), gp_send.at[o])

    for m in (1, 2) if relay else range(1, fs):
        piece = gathered.at[:, own_rows]
        remote(piece, piece, m_send.at[m - 1], m_recv.at[m - 1, 0, 0], f ^ m, t).wait_send()
    if relay:
        for m in (1, 2):
            piece = gathered.at[2 - m, own_rows]
            remote(piece, piece, r_send.at[m - 1], r_recv.at[m - 1, 0], f ^ m, t).wait_send()


MARKS = (13, 13, 14, 15, 16, 18)
FIRST = ((8, 8), (4, 1), (1, 4), (3, 3))


def final_kernel(*refs):
    first, second, step, weight, copy = refs[:5]
    outs, sem = refs[5:15], refs[15]
    moves = []
    for j in range(2):
        for k, source in enumerate((step, weight, copy, first, second)):
            moves.append((source.at[j], outs[5 * j + k]))
    moves = [pltpu.make_async_copy(a, b, sem.at[i]) for i, (a, b) in enumerate(moves)]
    for move in moves:
        move.start()
    for move in moves:
        move.wait()


def body(fs, tp, *args):
    saved_input, query_cot, _, query_master, key_master, query_basis, key_basis = args[:7]
    rows, rank = query_basis.shape
    tokens, columns = saved_input.shape
    width = query_cot.shape[1]
    part = rank // fs
    depth = tp // 2
    count = fs * rows
    half, chunk = tokens // 2, tokens // tp
    pieces = rows // min(rows, 128)
    hbm = pl.BlockSpec(memory_space=pltpu.HBM)
    vmem = pl.BlockSpec(memory_space=pltpu.VMEM)
    dma = pltpu.SemaphoreType.DMA
    own = pltpu.VMEM((2, rows, width), F32)
    moment = pltpu.VMEM((2, part, width), F32)
    pairs = [
        *(dma((1,)), dma((2, 2))),
        *(dma((1,)), dma((1,))),
        *(dma((1,)), dma((2,))),
        *(dma((1,)), dma((2,))),
        *(dma((1,)), dma((2, depth - 1))),
        *(dma((1,)), dma((2,))),
        *(dma((2, depth)), dma((depth, 2))),
        *(dma((depth,)), dma((depth,))),
        *(dma((1,)), dma((2, fs - 1))),
        *(dma((1,)), dma((2, fs - 1))),
        *(dma((1,)), dma((1,))),
    ]
    links = 2 if fs == 4 else fs - 1
    pairs += [dma((links,)), dma((links, 2, pieces)), dma((2,)), dma((2, pieces))]
    results = pl.pallas_call(
        functools.partial(exchange_kernel, fs, tp),
        name="exchange",
        out_shape=(moment, moment, own, own, pltpu.VMEM((2, count, width), BF)),
        in_specs=[hbm] * 11,
        out_specs=(vmem,) * 5,
        scratch_shapes=[
            pltpu.VMEM((2, count, rank), BF),
            pltpu.VMEM((2, count, width), BF),
            pltpu.VMEM((tokens, columns), BF),
            pltpu.VMEM((2, tokens, width), BF),
            pltpu.VMEM((2, rows, width), F32),
            pltpu.VMEM((4, part, width), F32),
            pltpu.VMEM((2, half, rank), BF),
            pltpu.VMEM((2, half, rank), BF),
            pltpu.VMEM((2, half, rank), F32),
            pltpu.VMEM((2, half, rank), BF),
            pltpu.VMEM((2, depth, chunk, rank), BF),
            pltpu.VMEM((2, tokens, rank), BF),
            pltpu.VMEM((2, rank, width), F32),
            pltpu.VMEM((2, rank, width), BF),
            pltpu.VMEM((2, fs, part, width), BF),
            pltpu.VMEM((2, part, width), BF),
            pltpu.VMEM((2, rank, width), BF),
            pltpu.VMEM((fs, -(-2 * width // HD // 8) * 8, HD), F32),
            pltpu.VMEM((2, 8, width), F32),
            dma((11,)),
            *pairs,
        ],
        compiler_params=pltpu.CompilerParams(
            collective_id=0, has_side_effects=True, vmem_limit_bytes=40 * 1024 * 1024
        ),
    )(*[pltpu.with_memory_space_constraint(a, pltpu.HBM) for a in args])

    big = jax.ShapeDtypeStruct((rows, width), F32)
    copied = jax.ShapeDtypeStruct((count, width), BF)
    small = jax.ShapeDtypeStruct((part, width), F32)
    return pl.pallas_call(
        final_kernel,
        name="final",
        out_shape=(big, big, copied, small, small) * 2,
        in_specs=[vmem] * 5,
        out_specs=(hbm,) * 10,
        scratch_shapes=[dma((10,))],
        compiler_params=pltpu.CompilerParams(vmem_limit_bytes=20 * 1024 * 1024),
    )(*results)


def solution(mesh):
    split, tall, wide = P("fs", "tp"), P("fs", None), P(None, "tp")
    outs = (split, split, wide, split, split)
    return jax.shard_map(
        functools.partial(body, mesh.shape["fs"], mesh.shape["tp"]),
        mesh=mesh,
        in_specs=(split,) * 5 + (tall, tall) + (split,) * 4,
        out_specs=outs + outs,
        check_vma=False,
    )
```

```python
import functools

import jax
import jax.numpy as jnp
from jax import lax
from jax.experimental import pallas as pl
from jax.experimental.pallas import tpu as pltpu
from jax.sharding import PartitionSpec as P

HD = 128

moment_decay = 0.8
square_decay = 0.9
square_floor = 1.0
norm_floor = 0.01
step_rate = 0.01

BF = jnp.bfloat16
F32 = jnp.float32
MESH = pl.DeviceIdType.MESH


def exchange_kernel(
    fs,
    tp,
    x_hbm,
    qc_hbm,
    kc_hbm,
    qm_hbm,
    km_hbm,
    qb_hbm,
    kb_hbm,
    qf_hbm,
    qs_hbm,
    kf_hbm,
    ks_hbm,
    first_new,
    second_new,
    step_ref,
    weight_ref,
    copy_ref,
    basis,
    gathered,
    x_v,
    cot,
    master,
    moment,
    half_send,
    half_recv,
    half_own,
    z_send,
    z_recv,
    low,
    proj,
    proj_send,
    proj_recv,
    proj_mid,
    ratio,
    sums,
    scales,
    load_sem,
    b_send,
    b_recv,
    d_send,
    d_recv,
    p_send,
    p_recv,
    zr_send,
    zr_recv,
    zg_send,
    zg_recv,
    pf_send,
    pf_recv,
    g_send,
    g_recv,
    gp_send,
    gp_recv,
    rs_send,
    rs_recv,
    ag_send,
    ag_recv,
    s_send,
    s_recv,
    m_send,
    m_recv,
    r_send,
    r_recv,
):
    f = lax.axis_index("fs")
    t = lax.axis_index("tp")
    z, c = t // 2, t % 2
    depth = tp // 2
    relay = fs == 4
    rows, rank = qb_hbm.shape
    width = qc_hbm.shape[1]
    tokens, columns = x_v.shape
    part = rank // fs
    half = tokens // 2
    chunk = tokens // tp
    group = rows // columns
    owner = t // group
    role = f ^ owner
    tile = min(rows, 256) // 2
    pieces = rows // tile

    def at(start, size):
        return pl.ds(pl.multiple_of(start, size), size)

    def remote(src, dst, send, recv, df, dt):
        return pltpu.make_async_remote_copy(
            src_ref=src,
            dst_ref=dst,
            send_sem=send,
            recv_sem=recv,
            device_id=(df, dt),
            device_id_type=MESH,
        )

    own_rows = at(f * rows, rows)
    sources = (
        (qb_hbm, basis.at[0, own_rows]),
        (kb_hbm, basis.at[1, own_rows]),
        (qm_hbm, master.at[0]),
        (km_hbm, master.at[1]),
        (x_hbm, x_v),
        (qc_hbm, cot.at[0]),
        (kc_hbm, cot.at[1]),
        (qf_hbm, moment.at[0]),
        (qs_hbm, moment.at[1]),
        (kf_hbm, moment.at[2]),
        (ks_hbm, moment.at[3]),
    )
    loads = [
        pltpu.make_async_copy(source, target, load_sem.at[(0, 1, 2, 3, 4, 5, 5, 6, 6, 6, 6)[i]])
        for i, (source, target) in enumerate(sources)
    ]
    for load in loads:
        load.start()

    barrier = pltpu.get_barrier_semaphore()
    for m in range(1, fs):
        pl.semaphore_signal(barrier, inc=1, device_id=(f ^ m, t), device_id_type=MESH)
    pl.semaphore_signal(barrier, inc=1, device_id=(f, t ^ 1), device_id_type=MESH)
    for d in range(1, depth):
        other = lax.rem(z + d, depth) * 2 + c
        pl.semaphore_signal(barrier, inc=1, device_id=(f, other), device_id_type=MESH)

    def master_copy(m, j, i):
        piece = gathered.at[j, at(f * rows + i * tile, tile)]
        return remote(piece, piece, m_send.at[m - 1], m_recv.at[m - 1, j, i // 2], f ^ m, t)

    def relay_copy(m, i):
        piece = gathered.at[2 - m, at((f ^ (3 - m)) * rows + i * tile, tile)]
        return remote(piece, piece, r_send.at[m - 1], r_recv.at[m - 1, i // 2], f ^ m, t)

    def master_wait(m, j, i):
        pair = gathered.at[j, at((f ^ m) * rows + i * 2 * tile, 2 * tile)]
        remote(pair, pair, m_send.at[m - 1], m_recv.at[m - 1, j, i], f ^ m, t).wait_recv()

    def relay_wait(m, i):
        pair = gathered.at[2 - m, at((f ^ 3) * rows + i * 2 * tile, 2 * tile)]
        remote(pair, pair, r_send.at[m - 1], r_recv.at[m - 1, i], f ^ m, t).wait_recv()

    def issue(m, start, stop):
        for turn in range(2):
            j = (m + 1 + turn) % 2
            low_end, high_end = max(start, turn * pieces), min(stop, (turn + 1) * pieces)
            if low_end < high_end:

                @pl.loop(low_end - turn * pieces, high_end - turn * pieces)
                def _(i, j=j):
                    master_copy(m, j, i).start()

        low_end, high_end = max(start, 2 * pieces), min(stop, 3 * pieces)
        if low_end < high_end:

            @pl.loop(low_end // 2 - pieces, high_end // 2 - pieces)
            def _(i):
                master_wait(3 - m, 2 - m, i)
                relay_copy(m, 2 * i).start()
                relay_copy(m, 2 * i + 1).start()

    def share(start, stop):
        for m in (1, 2):
            issue(m, start, stop)

    count = 3 * pieces
    marks = [count * k // 24 for k in MARKS]
    marks = [k if k <= 2 * pieces else k // 2 * 2 for k in marks]

    piece_rows = columns // 2

    def basis_copy(m, j, h, target):
        piece = basis.at[j, at(t * columns + h * piece_rows, piece_rows)]
        return remote(piece, piece, b_send.at[0], b_recv.at[j, h], target, t)

    loads[0].wait()
    loads[1].wait()
    pl.semaphore_wait(barrier, fs - 1 + depth)
    if relay:

        @pl.when(role == 0)
        def _():
            for j in range(2):
                basis_copy(0, j, 0, f ^ 1).start()
                basis_copy(0, j, 1, f ^ 2).start()
    else:

        @pl.when(role == 0)
        def _():
            for m in range(1, fs):
                for j in range(2):
                    for h in range(2):
                        basis_copy(m, j, h, f ^ m).start()

    for j in range(2):
        loads[2 + j].wait()

        @pl.loop(0, pieces)
        def _(i, j=j):
            gathered[j, at(f * rows + i * tile, tile), :] = master[j, at(i * tile, tile), :].astype(BF)

    if relay:
        first_marks = [[count * k // 24 for k in pair] for pair in FIRST]

        for k in range(4):

            @pl.when(role == k)
            def _(k=k):
                issue(1, 0, first_marks[k][0])
                issue(2, 0, first_marks[k][1])

        @pl.when(role == 1)
        def _():
            for j in range(2):
                basis_copy(0, j, 0, f ^ 2).wait_recv()
                basis_copy(0, j, 0, f ^ 2).start()

        @pl.when(role == 2)
        def _():
            for j in range(2):
                basis_copy(0, j, 1, f ^ 1).wait_recv()
                basis_copy(0, j, 1, f ^ 1).start()

        @pl.when(role == 3)
        def _():
            for j in range(2):
                basis_copy(0, j, 0, f ^ 1).wait_recv()
                basis_copy(0, j, 0, f ^ 1).start()
                basis_copy(0, j, 1, f ^ 2).wait_recv()
                basis_copy(0, j, 1, f ^ 2).start()

        for k in range(4):

            @pl.when(role == k)
            def _(k=k):
                issue(1, first_marks[k][0], marks[0])
                issue(2, first_marks[k][1], marks[0])
    else:
        for m in range(1, fs):
            for j in range(2):

                @pl.loop(0, pieces)
                def _(i, m=m, j=j):
                    master_copy(m, j, i).start()

    def basis_wait(j):
        if relay:

            @pl.when(role == 1)
            def _():
                basis_copy(0, j, 1, f).wait_recv()

            @pl.when(role == 2)
            def _():
                basis_copy(0, j, 0, f).wait_recv()
        else:

            @pl.when(role != 0)
            def _():
                for h in range(2):
                    basis_copy(0, j, h, f).wait_recv()

    def partner_copy(j):
        piece = basis.at[j, at(t * columns, columns)]
        return remote(piece, piece, d_send.at[0], d_recv.at[0], f, t ^ 1)

    step = min(half, 256)

    def project(start, j):
        return jnp.dot(
            x_v[at(start, step), :],
            basis[j, at(t * columns, columns), :],
            preferred_element_type=F32,
        )

    def swap(j):
        return remote(half_send.at[j], half_recv.at[j], p_send.at[0], p_recv.at[j], f, t ^ 1)

    def z_copy(j, d):
        other = lax.rem(z + d, depth)
        return remote(
            z_send.at[j, at(other * chunk, chunk)],
            z_recv.at[j, d],
            zr_send.at[0],
            zr_recv.at[j],
            f,
            other * 2 + c,
        )

    loads[4].wait()
    for j in range(2):
        basis_wait(j)

        @pl.loop(0, half // step)
        def _(i, j=j):
            half_send[j, at(i * step, step), :] = project((1 - c) * half + i * step, j).astype(BF)

        swap(j).start()

        @pl.loop(0, half // step)
        def _(i, j=j):
            half_own[j, at(i * step, step), :] = project(c * half + i * step, j)

        @pl.when(role != 0)
        def _(j=j):
            partner_copy(j).start()

        swap(j).wait_recv()

        @pl.loop(0, half // chunk)
        def _(i, j=j):
            place = at(i * chunk, chunk)
            both = half_own[j, place, :] + half_recv[j, place, :].astype(F32)
            half_own[j, place, :] = both
            z_send[j, place, :] = both.astype(BF)

        for d in range(1, depth):
            z_copy(j, d).start()

    def low_piece(j, d, core):
        return low.at[j, at(core * half + lax.rem(z + depth - d, depth) * chunk, chunk)]

    def g_copy(j, d):
        other = lax.rem(z + d, depth)
        return remote(
            low_piece(j, 0, c),
            low_piece(j, 0, c),
            zg_send.at[0],
            zg_recv.at[j, d - 1],
            f,
            other * 2 + c,
        )

    def forward(j, d):
        return remote(
            low_piece(j, d, c), low_piece(j, d, c), pf_send.at[0], pf_recv.at[j], f, t ^ 1
        )

    for j in range(2):
        total = half_own[j, at(z * chunk, chunk), :]
        received = z_recv.at[j, 1:depth]
        remote(received, received, zr_send.at[0], zr_recv.at[j], f, t ^ 1).wait_recv()
        for d in range(1, depth):
            total = total + z_recv[j, d].astype(F32)
        low[j, at(c * half + z * chunk, chunk), :] = total.astype(BF)
        for d in range(1, depth):
            g_copy(j, d).start()
        forward(j, 0).start()

    def block_copy(j, o, side, target):
        piece = basis.at[j, at((2 * o + c) * columns, columns)]
        return remote(
            piece, piece, g_send.at[side, o], g_recv.at[o, j], f, target * 2 + c
        )

    def block_forward(j, o):
        piece = basis.at[j, at((2 * o + c) * columns, columns)]
        return remote(piece, piece, gp_send.at[o], gp_recv.at[o], f, t ^ 1)

    def needed(o):
        return f != (2 * o) // group

    def spread(j, o, side):
        if side == 0:

            @pl.when(z >= 1)
            def _():
                block_copy(j, o, 0, z - 1).start()
        else:

            @pl.when(z <= depth - 2)
            def _():
                block_copy(j, o, 1, z + 1).start()

    @pl.when(needed(z))
    def _():
        for j in range(2):
            for side in range(2):
                spread(j, z, side)

    def arrive(s):
        for side in range(2):
            o = z + s if side == 0 else z - s
            inside = o <= depth - 1 if side == 0 else o >= 0

            @pl.when(inside & needed(o))
            def _(o=o, side=side):
                for j in range(2):
                    block_copy(j, o, side, z).wait_recv()
                    spread(j, o, side)
                    block_forward(j, o).start()

    pltpu.make_async_copy(cot, cot, load_sem.at[5]).wait()

    own = at(f * part, part)

    def project_low(j):
        for d in range(1, depth):
            g_copy(j, d).wait_recv()
            forward(j, d).start()
        received = low.at[j, at((1 - c) * half, half)]
        remote(received, received, pf_send.at[0], pf_recv.at[j], f, t ^ 1).wait_recv()
        product = lax.dot_general(
            low[j], cot[j], (((0,), (0,)), ((), ())), preferred_element_type=F32
        )
        proj[j] = product
        proj_send[j] = product.astype(BF)

    def update_moments(j, summed):
        first = moment_decay * moment[2 * j] + (1.0 - moment_decay) * summed
        second = square_decay * moment[2 * j + 1] + (1.0 - square_decay) * summed * summed
        first_new[j] = first
        second_new[j] = second
        ratio[j, own, :] = (first / jnp.sqrt(second + square_floor)).astype(BF)

    def reduce_copy(j, k):
        near, far = (1, 2) if j == 0 else (2, 1)
        if relay:
            source = proj_mid.at[j] if k == 3 else proj_send.at[j, at((f ^ (near, 3)[k - 1]) * part, part)]
            target = f ^ (far if k == 3 else near)
        else:
            source, target = proj_send.at[j, at((f ^ k) * part, part)], f ^ k
        return remote(
            source, proj_recv.at[j, k], rs_send.at[0], rs_recv.at[j, k - 1], target, t
        )

    def ratio_copy(j, k):
        near, far = (1, 2) if j == 0 else (2, 1)
        if relay:
            piece = ratio.at[j, at((f ^ near) * part, part) if k == 3 else own]
            target = f ^ (near if k == 1 else far)
        else:
            piece, target = ratio.at[j, own], f ^ k
        return remote(piece, piece, ag_send.at[0], ag_recv.at[j, k - 1], target, t)

    for j in range(2):
        project_low(j)
        for k in (2, 1) if relay else range(1, fs):
            reduce_copy(j, k).start()
        if relay:
            share(marks[j], marks[j + 1])

    if relay:
        for j in range(2):
            far = 2 if j == 0 else 1
            reduce_copy(j, 2).wait_recv()
            mid = proj[j, at((f ^ far) * part, part), :] + proj_recv[j, 2].astype(F32)
            proj_mid[j] = mid.astype(BF)
            reduce_copy(j, 3).start()
        share(marks[2], marks[3])
    arrive(1)
    pltpu.make_async_copy(moment, moment, load_sem.at[6]).wait()

    for j in range(2):
        summed = proj[j, own, :]
        for k in (1, 3) if relay else range(1, fs):
            reduce_copy(j, k).wait_recv()
            summed = summed + proj_recv[j, k].astype(F32)
        update_moments(j, summed)
        for k in (1, 2) if relay else range(1, fs):
            ratio_copy(j, k).start()
    if relay:
        share(marks[3], marks[4])
        for j in range(2):
            ratio_copy(j, 1).wait_recv()
            ratio_copy(j, 3).start()
        share(marks[4], marks[5])

    def ratio_wait(j):
        for k in (2, 3) if relay else range(1, fs):
            ratio_copy(j, k).wait_recv()

    if depth > 2:
        arrive(2)

    high = min(rows, 256)
    heads = width // HD
    sums[f] = jnp.zeros(sums.shape[1:], F32)
    for j in range(2):
        ratio_wait(j)

        def add(i, total, j=j):
            update = jnp.dot(
                basis[j, at(f * rows + i * high, high), :], ratio[j], preferred_element_type=F32
            )
            step_ref[j, at(i * high, high), :] = update
            return total + jnp.sum((update * update).reshape(high // 8, 8, width), axis=0)

        squares = lax.fori_loop(0, rows // high, add, jnp.zeros((8, width), F32))
        for h in range(heads):
            total = jnp.sum(squares[:, h * HD : (h + 1) * HD])
            sums[f, j * heads + h : j * heads + h + 1, :] = jnp.broadcast_to(total, (1, HD))

    def sums_copy(m):
        return remote(sums.at[f], sums.at[f], s_send.at[0], s_recv.at[0], f ^ m, t)

    for m in range(1, fs):
        sums_copy(m).start()
    if relay:
        share(marks[5], count)
    for s in range(3, depth):
        arrive(s)
    others = sums.at[0 : fs - 1]
    remote(others, others, s_send.at[0], s_recv.at[0], f ^ 1, t).wait_recv()
    total = sums[0]
    for k in range(1, fs):
        total = total + sums[k]
    factor = 1.0 / jnp.sqrt(total / (fs * rows * HD) + norm_floor)
    for j in range(2):
        for h in range(heads):
            row = factor[j * heads + h : j * heads + h + 1, :]
            scales[j, :, h * HD : (h + 1) * HD] = jnp.broadcast_to(row, (8, HD))

    def finish(j, place, update):
        change = update * (step_rate * scales[j, 0:1, :])
        copy_ref[j, place, :] = (gathered[j, place, :].astype(F32) - change).astype(BF)

    for j in range(2):

        @pl.loop(0, rows // high)
        def _(i, j=j):
            place = at(i * high, high)
            update = step_ref[j, place, :]
            finish(j, at(f * rows + i * high, high), update)
            step = update * scales[j, 0:1, :]
            step_ref[j, place, :] = step
            weight_ref[j, place, :] = master[j, place, :] - step_rate * step

    def both(o, core):
        return basis.at[:, at((2 * o + core) * columns, columns)]

    def partner_block():
        piece = both(z, 1 - c)
        return remote(piece, piece, d_send.at[0], d_recv.at[0], f, t ^ 1)

    @pl.when(role != 0)
    def _():
        partner_block().wait_recv()

    for s in range(1, depth):
        for o, inside in ((z + s, z + s <= depth - 1), (z - s, z - s >= 0)):

            @pl.when(inside & needed(o))
            def _(o=o):
                piece = both(o, 1 - c)
                remote(piece, piece, gp_send.at[o], gp_recv.at[o], f, t ^ 1).wait_recv()

    def finish_rows(j, start, size):
        place = at(start, size)
        update = jnp.dot(basis[j, place, :], ratio[j], preferred_element_type=F32)
        finish(j, place, update)

    large = min(rows, 512)
    pair = 2 * tile

    def finish_block(m, j, wait):
        @pl.loop(0, rows // large)
        def _(i):
            if wait:
                for k in range(large // pair):
                    master_wait(m, j, i * (large // pair) + k)
            finish_rows(j, (f ^ m) * rows + i * large, large)

    if relay:
        finish_block(1, 0, False)
        finish_block(2, 1, False)
        finish_block(1, 1, True)
        finish_block(2, 0, True)

        @pl.loop(0, rows // pair)
        def _(i):
            for m in (2, 1):
                relay_wait(m, i)
                finish_rows(2 - m, (f ^ 3) * rows + i * pair, pair)
    else:
        for m in range(1, fs):
            for j in range(2):
                finish_block(m, j, True)

    def sent(piece, sem):
        remote(piece, piece, sem, p_recv.at[0], f, t ^ 1).wait_send()

    if relay:
        for k in range(4):

            @pl.when(role == k)
            def _(k=k):
                sent(basis.at[:, 0 : columns if k in (0, 3) else piece_rows], b_send.at[0])
    else:

        @pl.when(role == 0)
        def _():
            for m in range(1, fs):
                sent(basis.at[:, 0:columns], b_send.at[0])

    @pl.when(role != 0)
    def _():
        sent(both(z, c), d_send.at[0])

    sent(half_send, p_send.at[0])
    sent(z_send.at[:, 0 : (depth - 1) * chunk], zr_send.at[0])
    sent(low.at[:, 0 : (depth - 1) * chunk], zg_send.at[0])
    sent(low.at[:, 0 : depth * chunk], pf_send.at[0])
    sent(proj_send.at[:, 0 : (fs - 1) * part], rs_send.at[0])
    sent(ratio.at[:, 0 : (fs - 1) * part], ag_send.at[0])
    sent(others, s_send.at[0])

    for s in range(depth):
        for side in range(2):
            o = z + s if side == 0 else z - s
            there = o <= depth - 1 if side == 0 else o >= 0
            inside = there & (z >= 1) if side == 0 else there & (z <= depth - 2)

            @pl.when(inside & needed(o))
            def _(o=o, side=side):
                sent(both(o, c), g_send.at[side, o])

            if s > 0:

                @pl.when(there & needed(o))
                def _(o=o):
                    sent(both(o, c), gp_send.at[o])

    for m in (1, 2) if relay else range(1, fs):
        piece = gathered.at[:, own_rows]
        remote(piece, piece, m_send.at[m - 1], m_recv.at[m - 1, 0, 0], f ^ m, t).wait_send()
    if relay:
        for m in (1, 2):
            piece = gathered.at[2 - m, own_rows]
            remote(piece, piece, r_send.at[m - 1], r_recv.at[m - 1, 0], f ^ m, t).wait_send()


MARKS = (14, 14, 15, 16, 18, 20)
FIRST = ((8, 8), (5, 2), (2, 5), (4, 4))


def final_kernel(*refs):
    first, second, step, weight, copy = refs[:5]
    outs, sem = refs[5:15], refs[15]
    moves = []
    for j in range(2):
        for k, source in enumerate((step, weight, copy, first, second)):
            moves.append((source.at[j], outs[5 * j + k]))
    moves = [pltpu.make_async_copy(a, b, sem.at[i]) for i, (a, b) in enumerate(moves)]
    for move in moves:
        move.start()
    for move in moves:
        move.wait()


def body(fs, tp, *args):
    saved_input, query_cot, _, query_master, key_master, query_basis, key_basis = args[:7]
    rows, rank = query_basis.shape
    tokens, columns = saved_input.shape
    width = query_cot.shape[1]
    part = rank // fs
    depth = tp // 2
    count = fs * rows
    half, chunk = tokens // 2, tokens // tp
    pieces = rows // (min(rows, 256) // 2)
    hbm = pl.BlockSpec(memory_space=pltpu.HBM)
    vmem = pl.BlockSpec(memory_space=pltpu.VMEM)
    dma = pltpu.SemaphoreType.DMA
    own = pltpu.VMEM((2, rows, width), F32)
    moment = pltpu.VMEM((2, part, width), F32)
    pairs = [
        *(dma((1,)), dma((2, 2))),
        *(dma((1,)), dma((1,))),
        *(dma((1,)), dma((2,))),
        *(dma((1,)), dma((2,))),
        *(dma((1,)), dma((2, depth - 1))),
        *(dma((1,)), dma((2,))),
        *(dma((2, depth)), dma((depth, 2))),
        *(dma((depth,)), dma((depth,))),
        *(dma((1,)), dma((2, fs - 1))),
        *(dma((1,)), dma((2, fs - 1))),
        *(dma((1,)), dma((1,))),
    ]
    links = 2 if fs == 4 else fs - 1
    pairs += [dma((links,)), dma((links, 2, pieces // 2)), dma((2,)), dma((2, pieces // 2))]
    results = pl.pallas_call(
        functools.partial(exchange_kernel, fs, tp),
        name="exchange",
        out_shape=(moment, moment, own, own, pltpu.VMEM((2, count, width), BF)),
        in_specs=[hbm] * 11,
        out_specs=(vmem,) * 5,
        scratch_shapes=[
            pltpu.VMEM((2, count, rank), BF),
            pltpu.VMEM((2, count, width), BF),
            pltpu.VMEM((tokens, columns), BF),
            pltpu.VMEM((2, tokens, width), BF),
            pltpu.VMEM((2, rows, width), F32),
            pltpu.VMEM((4, part, width), F32),
            pltpu.VMEM((2, half, rank), BF),
            pltpu.VMEM((2, half, rank), BF),
            pltpu.VMEM((2, half, rank), F32),
            pltpu.VMEM((2, half, rank), BF),
            pltpu.VMEM((2, depth, chunk, rank), BF),
            pltpu.VMEM((2, tokens, rank), BF),
            pltpu.VMEM((2, rank, width), F32),
            pltpu.VMEM((2, rank, width), BF),
            pltpu.VMEM((2, fs, part, width), BF),
            pltpu.VMEM((2, part, width), BF),
            pltpu.VMEM((2, rank, width), BF),
            pltpu.VMEM((fs, -(-2 * width // HD // 8) * 8, HD), F32),
            pltpu.VMEM((2, 8, width), F32),
            dma((7,)),
            *pairs,
        ],
        compiler_params=pltpu.CompilerParams(
            collective_id=0, has_side_effects=True, vmem_limit_bytes=40 * 1024 * 1024
        ),
    )(*[pltpu.with_memory_space_constraint(a, pltpu.HBM) for a in args])

    big = jax.ShapeDtypeStruct((rows, width), F32)
    copied = jax.ShapeDtypeStruct((count, width), BF)
    small = jax.ShapeDtypeStruct((part, width), F32)
    return pl.pallas_call(
        final_kernel,
        name="final",
        out_shape=(big, big, copied, small, small) * 2,
        in_specs=[vmem] * 5,
        out_specs=(hbm,) * 10,
        scratch_shapes=[dma((10,))],
        compiler_params=pltpu.CompilerParams(vmem_limit_bytes=20 * 1024 * 1024),
    )(*results)


def solution(mesh):
    split, tall, wide = P("fs", "tp"), P("fs", None), P(None, "tp")
    outs = (split, split, wide, split, split)
    return jax.shard_map(
        functools.partial(body, mesh.shape["fs"], mesh.shape["tp"]),
        mesh=mesh,
        in_specs=(split,) * 5 + (tall, tall) + (split,) * 4,
        out_specs=outs + outs,
        check_vma=False,
    )
```

```python
import functools

import jax
import jax.numpy as jnp
from jax import lax
from jax.experimental import pallas as pl
from jax.experimental.pallas import tpu as pltpu
from jax.sharding import PartitionSpec as P

HD = 128

moment_decay = 0.8
square_decay = 0.9
square_floor = 1.0
norm_floor = 0.01
step_rate = 0.01

BF = jnp.bfloat16
F32 = jnp.float32
MESH = pl.DeviceIdType.MESH


def exchange_kernel(
    fs,
    tp,
    x_hbm,
    qc_hbm,
    kc_hbm,
    qm_hbm,
    km_hbm,
    qb_hbm,
    kb_hbm,
    qf_hbm,
    qs_hbm,
    kf_hbm,
    ks_hbm,
    first_new,
    second_new,
    step_ref,
    weight_ref,
    copy_ref,
    basis,
    gathered,
    x_v,
    cot,
    master,
    moment,
    half_send,
    half_recv,
    half_own,
    z_send,
    z_recv,
    low,
    proj,
    proj_send,
    proj_recv,
    proj_mid,
    ratio,
    sums,
    scales,
    changes,
    load_sem,
    b_send,
    b_recv,
    d_send,
    d_recv,
    p_send,
    p_recv,
    zr_send,
    zr_recv,
    zg_send,
    zg_recv,
    pf_send,
    pf_recv,
    g_send,
    g_recv,
    gp_send,
    gp_recv,
    rs_send,
    rs_recv,
    ag_send,
    ag_recv,
    s_send,
    s_recv,
    m_send,
    m_recv,
    r_send,
    r_recv,
):
    f = lax.axis_index("fs")
    t = lax.axis_index("tp")
    z, c = t // 2, t % 2
    depth = tp // 2
    relay = fs == 4
    rows, rank = qb_hbm.shape
    width = qc_hbm.shape[1]
    tokens, columns = x_v.shape
    part = rank // fs
    half = tokens // 2
    chunk = tokens // tp
    group = rows // columns
    owner = t // group
    role = f ^ owner
    tile = min(rows, 256) // 2
    pieces = rows // tile

    def at(start, size):
        return pl.ds(pl.multiple_of(start, size), size)

    def remote(src, dst, send, recv, df, dt):
        return pltpu.make_async_remote_copy(
            src_ref=src,
            dst_ref=dst,
            send_sem=send,
            recv_sem=recv,
            device_id=(df, dt),
            device_id_type=MESH,
        )

    own_rows = at(f * rows, rows)
    sources = (
        (qb_hbm, basis.at[0, own_rows]),
        (kb_hbm, basis.at[1, own_rows]),
        (qm_hbm, master.at[0]),
        (km_hbm, master.at[1]),
        (x_hbm, x_v),
        (qc_hbm, cot.at[0]),
        (kc_hbm, cot.at[1]),
        (qf_hbm, moment.at[0]),
        (qs_hbm, moment.at[1]),
        (kf_hbm, moment.at[2]),
        (ks_hbm, moment.at[3]),
    )
    loads = [
        pltpu.make_async_copy(source, target, load_sem.at[(0, 1, 2, 3, 4, 5, 5, 6, 6, 6, 6)[i]])
        for i, (source, target) in enumerate(sources)
    ]
    for load in loads:
        load.start()

    barrier = pltpu.get_barrier_semaphore()
    for m in range(1, fs):
        pl.semaphore_signal(barrier, inc=1, device_id=(f ^ m, t), device_id_type=MESH)
    pl.semaphore_signal(barrier, inc=1, device_id=(f, t ^ 1), device_id_type=MESH)
    for d in range(1, depth):
        other = lax.rem(z + d, depth) * 2 + c
        pl.semaphore_signal(barrier, inc=1, device_id=(f, other), device_id_type=MESH)

    def master_copy(m, j, i):
        piece = gathered.at[j, at(f * rows + i * tile, tile)]
        return remote(piece, piece, m_send.at[m - 1], m_recv.at[m - 1, j, i // 2], f ^ m, t)

    def relay_copy(m, i):
        piece = gathered.at[2 - m, at((f ^ (3 - m)) * rows + i * tile, tile)]
        return remote(piece, piece, r_send.at[m - 1], r_recv.at[m - 1, i // 2], f ^ m, t)

    def master_wait(m, j, i):
        pair = gathered.at[j, at((f ^ m) * rows + i * 2 * tile, 2 * tile)]
        remote(pair, pair, m_send.at[m - 1], m_recv.at[m - 1, j, i], f ^ m, t).wait_recv()

    def relay_wait(m, i):
        pair = gathered.at[2 - m, at((f ^ 3) * rows + i * 2 * tile, 2 * tile)]
        remote(pair, pair, r_send.at[m - 1], r_recv.at[m - 1, i], f ^ m, t).wait_recv()

    def issue(m, start, stop):
        for turn in range(2):
            j = (m + 1 + turn) % 2
            low_end, high_end = max(start, turn * pieces), min(stop, (turn + 1) * pieces)
            if low_end < high_end:

                @pl.loop(low_end - turn * pieces, high_end - turn * pieces)
                def _(i, j=j):
                    master_copy(m, j, i).start()

        low_end, high_end = max(start, 2 * pieces), min(stop, 3 * pieces)
        if low_end < high_end:

            @pl.loop(low_end // 2 - pieces, high_end // 2 - pieces)
            def _(i):
                master_wait(3 - m, 2 - m, i)
                relay_copy(m, 2 * i).start()
                relay_copy(m, 2 * i + 1).start()

    def share(start, stop):
        for m in (1, 2):
            issue(m, start, stop)

    count = 3 * pieces
    marks = [count * k // 24 for k in MARKS]
    marks = [k if k <= 2 * pieces else k // 2 * 2 for k in marks]

    piece_rows = columns // 2

    def basis_copy(m, j, h, target):
        piece = basis.at[j, at(t * columns + h * piece_rows, piece_rows)]
        return remote(piece, piece, b_send.at[0], b_recv.at[j, h], target, t)

    loads[0].wait()
    loads[1].wait()
    early = z < depth // 2

    def round_masters():
        for j in range(2):
            loads[2 + j].wait()

            @pl.loop(0, pieces)
            def _(i, j=j):
                gathered[j, at(f * rows + i * tile, tile), :] = master[j, at(i * tile, tile), :].astype(BF)

    pl.when(early)(round_masters)
    pl.semaphore_wait(barrier, fs - 1 + depth)
    if relay:

        @pl.when(role == 0)
        def _():
            for j in range(2):
                basis_copy(0, j, 0, f ^ 1).start()
                basis_copy(0, j, 1, f ^ 2).start()
    else:

        @pl.when(role == 0)
        def _():
            for m in range(1, fs):
                for j in range(2):
                    for h in range(2):
                        basis_copy(m, j, h, f ^ m).start()

    pl.when(jnp.logical_not(early))(round_masters)
    if relay:
        first_marks = [[count * k // 24 for k in pair] for pair in FIRST]

        for k in range(4):

            @pl.when(role == k)
            def _(k=k):
                issue(1, 0, first_marks[k][0])
                issue(2, 0, first_marks[k][1])

        @pl.when(role == 1)
        def _():
            for j in range(2):
                basis_copy(0, j, 0, f ^ 2).wait_recv()
                basis_copy(0, j, 0, f ^ 2).start()

        @pl.when(role == 2)
        def _():
            for j in range(2):
                basis_copy(0, j, 1, f ^ 1).wait_recv()
                basis_copy(0, j, 1, f ^ 1).start()

        @pl.when(role == 3)
        def _():
            for j in range(2):
                basis_copy(0, j, 0, f ^ 1).wait_recv()
                basis_copy(0, j, 0, f ^ 1).start()
                basis_copy(0, j, 1, f ^ 2).wait_recv()
                basis_copy(0, j, 1, f ^ 2).start()

        for k in range(4):

            @pl.when(role == k)
            def _(k=k):
                issue(1, first_marks[k][0], marks[0])
                issue(2, first_marks[k][1], marks[0])
    else:
        for m in range(1, fs):
            for j in range(2):

                @pl.loop(0, pieces)
                def _(i, m=m, j=j):
                    master_copy(m, j, i).start()

    def basis_wait(j):
        if relay:

            @pl.when(role == 1)
            def _():
                basis_copy(0, j, 1, f).wait_recv()

            @pl.when(role == 2)
            def _():
                basis_copy(0, j, 0, f).wait_recv()
        else:

            @pl.when(role != 0)
            def _():
                for h in range(2):
                    basis_copy(0, j, h, f).wait_recv()

    def partner_copy(j):
        piece = basis.at[j, at(t * columns, columns)]
        return remote(piece, piece, d_send.at[0], d_recv.at[0], f, t ^ 1)

    step = min(half, 256)

    def project(start, j):
        return jnp.dot(
            x_v[at(start, step), :],
            basis[j, at(t * columns, columns), :],
            preferred_element_type=F32,
        )

    def swap(j):
        return remote(half_send.at[j], half_recv.at[j], p_send.at[0], p_recv.at[j], f, t ^ 1)

    def z_copy(j, d):
        other = lax.rem(z + d, depth)
        return remote(
            z_send.at[j, at(other * chunk, chunk)],
            z_recv.at[j, d],
            zr_send.at[0],
            zr_recv.at[j],
            f,
            other * 2 + c,
        )

    loads[4].wait()
    for j in range(2):
        basis_wait(j)

        @pl.loop(0, half // step)
        def _(i, j=j):
            half_send[j, at(i * step, step), :] = project((1 - c) * half + i * step, j).astype(BF)

        swap(j).start()

        @pl.loop(0, half // step)
        def _(i, j=j):
            half_own[j, at(i * step, step), :] = project(c * half + i * step, j)

        @pl.when(role != 0)
        def _(j=j):
            partner_copy(j).start()

        swap(j).wait_recv()

        @pl.loop(0, half // chunk)
        def _(i, j=j):
            place = at(i * chunk, chunk)
            both = half_own[j, place, :] + half_recv[j, place, :].astype(F32)
            half_own[j, place, :] = both
            z_send[j, place, :] = both.astype(BF)

        for d in range(1, depth):
            z_copy(j, d).start()

    def low_piece(j, d, core):
        return low.at[j, at(core * half + lax.rem(z + depth - d, depth) * chunk, chunk)]

    def g_copy(j, d):
        other = lax.rem(z + d, depth)
        return remote(
            low_piece(j, 0, c),
            low_piece(j, 0, c),
            zg_send.at[0],
            zg_recv.at[j, d - 1],
            f,
            other * 2 + c,
        )

    def forward(j, d):
        return remote(
            low_piece(j, d, c), low_piece(j, d, c), pf_send.at[0], pf_recv.at[j], f, t ^ 1
        )

    for j in range(2):
        total = half_own[j, at(z * chunk, chunk), :]
        received = z_recv.at[j, 1:depth]
        remote(received, received, zr_send.at[0], zr_recv.at[j], f, t ^ 1).wait_recv()
        for d in range(1, depth):
            total = total + z_recv[j, d].astype(F32)
        low[j, at(c * half + z * chunk, chunk), :] = total.astype(BF)
        for d in range(1, depth):
            g_copy(j, d).start()
        forward(j, 0).start()

    def block_copy(j, o, side, target):
        piece = basis.at[j, at((2 * o + c) * columns, columns)]
        return remote(
            piece, piece, g_send.at[side, o], g_recv.at[o, j], f, target * 2 + c
        )

    def block_forward(j, o):
        piece = basis.at[j, at((2 * o + c) * columns, columns)]
        return remote(piece, piece, gp_send.at[o], gp_recv.at[o], f, t ^ 1)

    def needed(o):
        return f != (2 * o) // group

    def spread(j, o, side):
        if side == 0:

            @pl.when(z >= 1)
            def _():
                block_copy(j, o, 0, z - 1).start()
        else:

            @pl.when(z <= depth - 2)
            def _():
                block_copy(j, o, 1, z + 1).start()

    @pl.when(needed(z))
    def _():
        for j in range(2):
            for side in range(2):
                spread(j, z, side)

    def arrive(s):
        for side in range(2):
            o = z + s if side == 0 else z - s
            inside = o <= depth - 1 if side == 0 else o >= 0

            @pl.when(inside & needed(o))
            def _(o=o, side=side):
                for j in range(2):
                    block_copy(j, o, side, z).wait_recv()
                    spread(j, o, side)
                    block_forward(j, o).start()

    pltpu.make_async_copy(cot, cot, load_sem.at[5]).wait()

    own = at(f * part, part)

    def project_low(j):
        for d in range(1, depth):
            g_copy(j, d).wait_recv()
            forward(j, d).start()
        received = low.at[j, at((1 - c) * half, half)]
        remote(received, received, pf_send.at[0], pf_recv.at[j], f, t ^ 1).wait_recv()
        product = lax.dot_general(
            low[j], cot[j], (((0,), (0,)), ((), ())), preferred_element_type=F32
        )
        proj[j] = product
        proj_send[j] = product.astype(BF)

    def update_moments(j, summed):
        first = moment_decay * moment[2 * j] + (1.0 - moment_decay) * summed
        second = square_decay * moment[2 * j + 1] + (1.0 - square_decay) * summed * summed
        first_new[j] = first
        second_new[j] = second
        ratio[j, own, :] = (first / jnp.sqrt(second + square_floor)).astype(BF)

    def reduce_copy(j, k):
        near, far = (1, 2) if j == 0 else (2, 1)
        if relay:
            source = proj_mid.at[j] if k == 3 else proj_send.at[j, at((f ^ (near, 3)[k - 1]) * part, part)]
            target = f ^ (far if k == 3 else near)
        else:
            source, target = proj_send.at[j, at((f ^ k) * part, part)], f ^ k
        return remote(
            source, proj_recv.at[j, k], rs_send.at[0], rs_recv.at[j, k - 1], target, t
        )

    def ratio_copy(j, k):
        near, far = (1, 2) if j == 0 else (2, 1)
        if relay:
            piece = ratio.at[j, at((f ^ near) * part, part) if k == 3 else own]
            target = f ^ (near if k == 1 else far)
        else:
            piece, target = ratio.at[j, own], f ^ k
        return remote(piece, piece, ag_send.at[0], ag_recv.at[j, k - 1], target, t)

    for j in range(2):
        project_low(j)
        for k in (2, 1) if relay else range(1, fs):
            reduce_copy(j, k).start()
        if relay:
            share(marks[j], marks[j + 1])

    if relay:
        for j in range(2):
            far = 2 if j == 0 else 1
            reduce_copy(j, 2).wait_recv()
            mid = proj[j, at((f ^ far) * part, part), :] + proj_recv[j, 2].astype(F32)
            proj_mid[j] = mid.astype(BF)
            reduce_copy(j, 3).start()
        share(marks[2], marks[3])
    arrive(1)
    pltpu.make_async_copy(moment, moment, load_sem.at[6]).wait()

    for j in range(2):
        summed = proj[j, own, :]
        for k in (1, 3) if relay else range(1, fs):
            reduce_copy(j, k).wait_recv()
            summed = summed + proj_recv[j, k].astype(F32)
        update_moments(j, summed)
        for k in (1, 2) if relay else range(1, fs):
            ratio_copy(j, k).start()
    if relay:
        share(marks[3], marks[4])
        for j in range(2):
            ratio_copy(j, 1).wait_recv()
            ratio_copy(j, 3).start()
        share(marks[4], marks[5])

    def ratio_wait(j):
        for k in (2, 3) if relay else range(1, fs):
            ratio_copy(j, k).wait_recv()

    if depth > 2:
        arrive(2)

    high = min(rows, 256)
    heads = width // HD
    sums[f] = jnp.zeros(sums.shape[1:], F32)
    for j in range(2):
        ratio_wait(j)

        def add(i, total, j=j):
            update = jnp.dot(
                basis[j, at(f * rows + i * high, high), :], ratio[j], preferred_element_type=F32
            )
            step_ref[j, at(i * high, high), :] = update
            return total + jnp.sum((update * update).reshape(high // 8, 8, width), axis=0)

        squares = lax.fori_loop(0, rows // high, add, jnp.zeros((8, width), F32))
        for h in range(heads):
            total = jnp.sum(squares[:, h * HD : (h + 1) * HD])
            sums[f, j * heads + h : j * heads + h + 1, :] = jnp.broadcast_to(total, (1, HD))

    def sums_copy(m):
        return remote(sums.at[f], sums.at[f], s_send.at[0], s_recv.at[0], f ^ m, t)

    for m in range(1, fs):
        sums_copy(m).start()
    if relay:
        share(marks[5], count)
    for s in range(3, depth):
        arrive(s)
    others = sums.at[0 : fs - 1]
    remote(others, others, s_send.at[0], s_recv.at[0], f ^ 1, t).wait_recv()
    total = sums[0]
    for k in range(1, fs):
        total = total + sums[k]
    factor = 1.0 / jnp.sqrt(total / (fs * rows * HD) + norm_floor)
    for j in range(2):
        for h in range(heads):
            row = factor[j * heads + h : j * heads + h + 1, :]
            scales[j, :, h * HD : (h + 1) * HD] = jnp.broadcast_to(row, (8, HD))

    def finish(j, place, update):
        change = update * (step_rate * scales[j, 0:1, :])
        copy_ref[j, place, :] = (gathered[j, place, :].astype(F32) - change).astype(BF)

    for j in range(2):

        @pl.loop(0, rows // high)
        def _(i, j=j):
            place = at(i * high, high)
            update = step_ref[j, place, :]
            finish(j, at(f * rows + i * high, high), update)
            step = update * scales[j, 0:1, :]
            step_ref[j, place, :] = step
            weight_ref[j, place, :] = master[j, place, :] - step_rate * step

    def both(o, core):
        return basis.at[:, at((2 * o + core) * columns, columns)]

    def partner_block():
        piece = both(z, 1 - c)
        return remote(piece, piece, d_send.at[0], d_recv.at[0], f, t ^ 1)

    @pl.when(role != 0)
    def _():
        partner_block().wait_recv()

    for s in range(1, depth):
        for o, inside in ((z + s, z + s <= depth - 1), (z - s, z - s >= 0)):

            @pl.when(inside & needed(o))
            def _(o=o):
                piece = both(o, 1 - c)
                remote(piece, piece, gp_send.at[o], gp_recv.at[o], f, t ^ 1).wait_recv()

    def finish_rows(j, start, size):
        place = at(start, size)
        update = jnp.dot(basis[j, place, :], ratio[j], preferred_element_type=F32)
        finish(j, place, update)

    large = min(rows, 512)
    pair = 2 * tile

    def finish_block(m, j, wait):
        @pl.loop(0, rows // large)
        def _(i):
            if wait:
                for k in range(large // pair):
                    master_wait(m, j, i * (large // pair) + k)
            finish_rows(j, (f ^ m) * rows + i * large, large)

    if relay:
        finish_block(1, 0, False)
        finish_block(2, 1, False)
        finish_block(1, 1, True)
        finish_block(2, 0, True)

        @pl.loop(0, rows // pair)
        def _(i):
            place = at((f ^ 3) * rows + i * pair, pair)
            for j in range(2):
                update = jnp.dot(basis[j, place, :], ratio[j], preferred_element_type=F32)
                changes[j] = update * (step_rate * scales[j, 0:1, :])
            for j in range(2):
                relay_wait(2 - j, i)
                copy_ref[j, place, :] = (gathered[j, place, :].astype(F32) - changes[j]).astype(BF)
    else:
        for m in range(1, fs):
            for j in range(2):
                finish_block(m, j, True)

    def sent(piece, sem):
        remote(piece, piece, sem, p_recv.at[0], f, t ^ 1).wait_send()

    if relay:
        for k in range(4):

            @pl.when(role == k)
            def _(k=k):
                sent(basis.at[:, 0 : columns if k in (0, 3) else piece_rows], b_send.at[0])
    else:

        @pl.when(role == 0)
        def _():
            for m in range(1, fs):
                sent(basis.at[:, 0:columns], b_send.at[0])

    @pl.when(role != 0)
    def _():
        sent(both(z, c), d_send.at[0])

    sent(half_send, p_send.at[0])
    sent(z_send.at[:, 0 : (depth - 1) * chunk], zr_send.at[0])
    sent(low.at[:, 0 : (depth - 1) * chunk], zg_send.at[0])
    sent(low.at[:, 0 : depth * chunk], pf_send.at[0])
    sent(proj_send.at[:, 0 : (fs - 1) * part], rs_send.at[0])
    sent(ratio.at[:, 0 : (fs - 1) * part], ag_send.at[0])
    sent(others, s_send.at[0])

    for s in range(depth):
        for side in range(2):
            o = z + s if side == 0 else z - s
            there = o <= depth - 1 if side == 0 else o >= 0
            inside = there & (z >= 1) if side == 0 else there & (z <= depth - 2)

            @pl.when(inside & needed(o))
            def _(o=o, side=side):
                sent(both(o, c), g_send.at[side, o])

            if s > 0:

                @pl.when(there & needed(o))
                def _(o=o):
                    sent(both(o, c), gp_send.at[o])

    for m in (1, 2) if relay else range(1, fs):
        piece = gathered.at[:, own_rows]
        remote(piece, piece, m_send.at[m - 1], m_recv.at[m - 1, 0, 0], f ^ m, t).wait_send()
    if relay:
        for m in (1, 2):
            piece = gathered.at[2 - m, own_rows]
            remote(piece, piece, r_send.at[m - 1], r_recv.at[m - 1, 0], f ^ m, t).wait_send()


MARKS = (14, 14, 15, 16, 18, 20)
FIRST = ((8, 8), (5, 2), (2, 5), (4, 4))


def final_kernel(*refs):
    first, second, step, weight, copy = refs[:5]
    outs, sem = refs[5:15], refs[15]
    moves = []
    for j in range(2):
        for k, source in enumerate((step, weight, copy, first, second)):
            moves.append((source.at[j], outs[5 * j + k]))
    moves = [pltpu.make_async_copy(a, b, sem.at[i]) for i, (a, b) in enumerate(moves)]
    for move in moves:
        move.start()
    for move in moves:
        move.wait()


def body(fs, tp, *args):
    saved_input, query_cot, _, query_master, key_master, query_basis, key_basis = args[:7]
    rows, rank = query_basis.shape
    tokens, columns = saved_input.shape
    width = query_cot.shape[1]
    part = rank // fs
    depth = tp // 2
    count = fs * rows
    half, chunk = tokens // 2, tokens // tp
    pieces = rows // (min(rows, 256) // 2)
    hbm = pl.BlockSpec(memory_space=pltpu.HBM)
    vmem = pl.BlockSpec(memory_space=pltpu.VMEM)
    dma = pltpu.SemaphoreType.DMA
    own = pltpu.VMEM((2, rows, width), F32)
    moment = pltpu.VMEM((2, part, width), F32)
    pairs = [
        *(dma((1,)), dma((2, 2))),
        *(dma((1,)), dma((1,))),
        *(dma((1,)), dma((2,))),
        *(dma((1,)), dma((2,))),
        *(dma((1,)), dma((2, depth - 1))),
        *(dma((1,)), dma((2,))),
        *(dma((2, depth)), dma((depth, 2))),
        *(dma((depth,)), dma((depth,))),
        *(dma((1,)), dma((2, fs - 1))),
        *(dma((1,)), dma((2, fs - 1))),
        *(dma((1,)), dma((1,))),
    ]
    links = 2 if fs == 4 else fs - 1
    pairs += [dma((links,)), dma((links, 2, pieces // 2)), dma((2,)), dma((2, pieces // 2))]
    results = pl.pallas_call(
        functools.partial(exchange_kernel, fs, tp),
        name="exchange",
        out_shape=(moment, moment, own, own, pltpu.VMEM((2, count, width), BF)),
        in_specs=[hbm] * 11,
        out_specs=(vmem,) * 5,
        scratch_shapes=[
            pltpu.VMEM((2, count, rank), BF),
            pltpu.VMEM((2, count, width), BF),
            pltpu.VMEM((tokens, columns), BF),
            pltpu.VMEM((2, tokens, width), BF),
            pltpu.VMEM((2, rows, width), F32),
            pltpu.VMEM((4, part, width), F32),
            pltpu.VMEM((2, half, rank), BF),
            pltpu.VMEM((2, half, rank), BF),
            pltpu.VMEM((2, half, rank), F32),
            pltpu.VMEM((2, half, rank), BF),
            pltpu.VMEM((2, depth, chunk, rank), BF),
            pltpu.VMEM((2, tokens, rank), BF),
            pltpu.VMEM((2, rank, width), F32),
            pltpu.VMEM((2, rank, width), BF),
            pltpu.VMEM((2, fs, part, width), BF),
            pltpu.VMEM((2, part, width), BF),
            pltpu.VMEM((2, rank, width), BF),
            pltpu.VMEM((fs, -(-2 * width // HD // 8) * 8, HD), F32),
            pltpu.VMEM((2, 8, width), F32),
            pltpu.VMEM((2, min(rows, 256), width), F32),
            dma((7,)),
            *pairs,
        ],
        compiler_params=pltpu.CompilerParams(
            collective_id=0, has_side_effects=True, vmem_limit_bytes=40 * 1024 * 1024
        ),
    )(*[pltpu.with_memory_space_constraint(a, pltpu.HBM) for a in args])

    big = jax.ShapeDtypeStruct((rows, width), F32)
    copied = jax.ShapeDtypeStruct((count, width), BF)
    small = jax.ShapeDtypeStruct((part, width), F32)
    return pl.pallas_call(
        final_kernel,
        name="final",
        out_shape=(big, big, copied, small, small) * 2,
        in_specs=[vmem] * 5,
        out_specs=(hbm,) * 10,
        scratch_shapes=[dma((10,))],
        compiler_params=pltpu.CompilerParams(vmem_limit_bytes=20 * 1024 * 1024),
    )(*results)


def solution(mesh):
    split, tall, wide = P("fs", "tp"), P("fs", None), P(None, "tp")
    outs = (split, split, wide, split, split)
    return jax.shard_map(
        functools.partial(body, mesh.shape["fs"], mesh.shape["tp"]),
        mesh=mesh,
        in_specs=(split,) * 5 + (tall, tall) + (split,) * 4,
        out_specs=outs + outs,
        check_vma=False,
    )
```

```python
import functools

import jax
import jax.numpy as jnp
from jax import lax
from jax.experimental import pallas as pl
from jax.experimental.pallas import tpu as pltpu
from jax.sharding import PartitionSpec as P

HD = 128

moment_decay = 0.8
square_decay = 0.9
square_floor = 1.0
norm_floor = 0.01
step_rate = 0.01

BF = jnp.bfloat16
F32 = jnp.float32
MESH = pl.DeviceIdType.MESH


def exchange_kernel(
    fs,
    tp,
    x_hbm,
    qc_hbm,
    kc_hbm,
    qm_hbm,
    km_hbm,
    qb_hbm,
    kb_hbm,
    qf_hbm,
    qs_hbm,
    kf_hbm,
    ks_hbm,
    first_new,
    second_new,
    step_ref,
    weight_ref,
    copy_ref,
    basis,
    gathered,
    x_v,
    cot,
    master,
    moment,
    half_send,
    half_recv,
    half_own,
    z_send,
    z_recv,
    low,
    proj,
    proj_send,
    proj_recv,
    proj_mid,
    ratio,
    sums,
    scales,
    changes,
    load_sem,
    b_send,
    b_recv,
    d_send,
    d_recv,
    p_send,
    p_recv,
    zr_send,
    zr_recv,
    zg_send,
    zg_recv,
    pf_send,
    pf_recv,
    g_send,
    g_recv,
    gp_send,
    gp_recv,
    rs_send,
    rs_recv,
    ag_send,
    ag_recv,
    s_send,
    s_recv,
    m_send,
    m_recv,
    r_send,
    r_recv,
):
    f = lax.axis_index("fs")
    t = lax.axis_index("tp")
    z, c = t // 2, t % 2
    depth = tp // 2
    relay = fs == 4
    rows, rank = qb_hbm.shape
    width = qc_hbm.shape[1]
    tokens, columns = x_v.shape
    part = rank // fs
    half = tokens // 2
    chunk = tokens // tp
    group = rows // columns
    owner = t // group
    role = f ^ owner
    tile = min(rows, 256) // 2
    pieces = rows // tile

    def at(start, size):
        return pl.ds(pl.multiple_of(start, size), size)

    def remote(src, dst, send, recv, df, dt):
        return pltpu.make_async_remote_copy(
            src_ref=src,
            dst_ref=dst,
            send_sem=send,
            recv_sem=recv,
            device_id=(df, dt),
            device_id_type=MESH,
        )

    own_rows = at(f * rows, rows)
    sources = (
        (qb_hbm, basis.at[0, own_rows]),
        (kb_hbm, basis.at[1, own_rows]),
        (qm_hbm, master.at[0]),
        (km_hbm, master.at[1]),
        (x_hbm, x_v),
        (qc_hbm, cot.at[0]),
        (kc_hbm, cot.at[1]),
        (qf_hbm, moment.at[0]),
        (qs_hbm, moment.at[1]),
        (kf_hbm, moment.at[2]),
        (ks_hbm, moment.at[3]),
    )
    loads = [
        pltpu.make_async_copy(source, target, load_sem.at[(0, 1, 2, 3, 4, 5, 5, 6, 6, 6, 6)[i]])
        for i, (source, target) in enumerate(sources)
    ]
    for load in loads:
        load.start()

    barrier = pltpu.get_barrier_semaphore()
    for m in range(1, fs):
        pl.semaphore_signal(barrier, inc=1, device_id=(f ^ m, t), device_id_type=MESH)
    pl.semaphore_signal(barrier, inc=1, device_id=(f, t ^ 1), device_id_type=MESH)
    for d in range(1, depth):
        other = lax.rem(z + d, depth) * 2 + c
        pl.semaphore_signal(barrier, inc=1, device_id=(f, other), device_id_type=MESH)

    def master_copy(m, j, i):
        piece = gathered.at[j, at(f * rows + i * tile, tile)]
        return remote(piece, piece, m_send.at[m - 1], m_recv.at[m - 1, j, i // 2], f ^ m, t)

    def relay_copy(m, i):
        piece = gathered.at[2 - m, at((f ^ (3 - m)) * rows + i * tile, tile)]
        return remote(piece, piece, r_send.at[m - 1], r_recv.at[m - 1, i // 2], f ^ m, t)

    def master_wait(m, j, i):
        pair = gathered.at[j, at((f ^ m) * rows + i * 2 * tile, 2 * tile)]
        remote(pair, pair, m_send.at[m - 1], m_recv.at[m - 1, j, i], f ^ m, t).wait_recv()

    def relay_wait(m, i):
        pair = gathered.at[2 - m, at((f ^ 3) * rows + i * 2 * tile, 2 * tile)]
        remote(pair, pair, r_send.at[m - 1], r_recv.at[m - 1, i], f ^ m, t).wait_recv()

    def issue(m, start, stop):
        for turn in range(2):
            j = (m + 1 + turn) % 2
            low_end, high_end = max(start, turn * pieces), min(stop, (turn + 1) * pieces)
            if low_end < high_end:

                @pl.loop(low_end - turn * pieces, high_end - turn * pieces)
                def _(i, j=j):
                    master_copy(m, j, i).start()

        low_end, high_end = max(start, 2 * pieces), min(stop, 3 * pieces)
        if low_end < high_end:

            @pl.loop(low_end // 2 - pieces, high_end // 2 - pieces)
            def _(i):
                master_wait(3 - m, 2 - m, i)
                relay_copy(m, 2 * i).start()
                relay_copy(m, 2 * i + 1).start()

    def share(start, stop):
        for m in (1, 2):
            issue(m, start, stop)

    count = 3 * pieces
    marks = [count * k // 24 for k in MARKS]
    marks = [k if k <= 2 * pieces else k // 2 * 2 for k in marks]

    piece_rows = columns // 2

    def basis_copy(m, j, h, target):
        piece = basis.at[j, at(t * columns + h * piece_rows, piece_rows)]
        return remote(piece, piece, b_send.at[0], b_recv.at[j, h], target, t)

    loads[0].wait()
    loads[1].wait()
    early = z < depth // 2

    def round_masters():
        for j in range(2):
            loads[2 + j].wait()

            @pl.loop(0, pieces)
            def _(i, j=j):
                gathered[j, at(f * rows + i * tile, tile), :] = master[j, at(i * tile, tile), :].astype(BF)

    pl.when(early)(round_masters)
    pl.semaphore_wait(barrier, fs - 1 + depth)
    if relay:

        @pl.when(role == 0)
        def _():
            for j in range(2):
                basis_copy(0, j, 0, f ^ 1).start()
                basis_copy(0, j, 1, f ^ 2).start()
    else:

        @pl.when(role == 0)
        def _():
            for m in range(1, fs):
                for j in range(2):
                    for h in range(2):
                        basis_copy(m, j, h, f ^ m).start()

    pl.when(jnp.logical_not(early))(round_masters)
    if relay:
        first_marks = [[count * k // 24 for k in pair] for pair in FIRST]

        for k in range(4):

            @pl.when(role == k)
            def _(k=k):
                issue(1, 0, first_marks[k][0])
                issue(2, 0, first_marks[k][1])

        @pl.when(role == 1)
        def _():
            for j in range(2):
                basis_copy(0, j, 0, f ^ 2).wait_recv()
                basis_copy(0, j, 0, f ^ 2).start()

        @pl.when(role == 2)
        def _():
            for j in range(2):
                basis_copy(0, j, 1, f ^ 1).wait_recv()
                basis_copy(0, j, 1, f ^ 1).start()

        @pl.when(role == 3)
        def _():
            for j in range(2):
                basis_copy(0, j, 0, f ^ 1).wait_recv()
                basis_copy(0, j, 0, f ^ 1).start()
                basis_copy(0, j, 1, f ^ 2).wait_recv()
                basis_copy(0, j, 1, f ^ 2).start()

        for k in range(4):

            @pl.when(role == k)
            def _(k=k):
                issue(1, first_marks[k][0], marks[0])
                issue(2, first_marks[k][1], marks[0])
    else:
        for m in range(1, fs):
            for j in range(2):

                @pl.loop(0, pieces)
                def _(i, m=m, j=j):
                    master_copy(m, j, i).start()

    def basis_wait(j):
        if relay:

            @pl.when(role == 1)
            def _():
                basis_copy(0, j, 1, f).wait_recv()

            @pl.when(role == 2)
            def _():
                basis_copy(0, j, 0, f).wait_recv()
        else:

            @pl.when(role != 0)
            def _():
                for h in range(2):
                    basis_copy(0, j, h, f).wait_recv()

    def partner_copy(j):
        piece = basis.at[j, at(t * columns, columns)]
        return remote(piece, piece, d_send.at[0], d_recv.at[0], f, t ^ 1)

    step = min(half, 256)

    def project(start, j):
        return jnp.dot(
            x_v[at(start, step), :],
            basis[j, at(t * columns, columns), :],
            preferred_element_type=F32,
        )

    def swap(j):
        return remote(half_send.at[j], half_recv.at[j], p_send.at[0], p_recv.at[j], f, t ^ 1)

    def z_copy(j, d):
        other = lax.rem(z + d, depth)
        return remote(
            z_send.at[j, at(other * chunk, chunk)],
            z_recv.at[j, d],
            zr_send.at[0],
            zr_recv.at[j],
            f,
            other * 2 + c,
        )

    loads[4].wait()
    for j in range(2):
        basis_wait(j)

        @pl.loop(0, half // step)
        def _(i, j=j):
            half_send[j, at(i * step, step), :] = project((1 - c) * half + i * step, j).astype(BF)

        swap(j).start()

        @pl.loop(0, half // step)
        def _(i, j=j):
            half_own[j, at(i * step, step), :] = project(c * half + i * step, j)

        @pl.when(role != 0)
        def _(j=j):
            partner_copy(j).start()

        swap(j).wait_recv()

        @pl.loop(0, half // chunk)
        def _(i, j=j):
            place = at(i * chunk, chunk)
            both = half_own[j, place, :] + half_recv[j, place, :].astype(F32)
            half_own[j, place, :] = both
            z_send[j, place, :] = both.astype(BF)

        for d in range(1, depth):
            z_copy(j, d).start()

    def low_piece(j, d, core):
        return low.at[j, at(core * half + lax.rem(z + depth - d, depth) * chunk, chunk)]

    def g_copy(j, d):
        other = lax.rem(z + d, depth)
        return remote(
            low_piece(j, 0, c),
            low_piece(j, 0, c),
            zg_send.at[0],
            zg_recv.at[j, d - 1],
            f,
            other * 2 + c,
        )

    def forward(j, d):
        return remote(
            low_piece(j, d, c), low_piece(j, d, c), pf_send.at[0], pf_recv.at[j], f, t ^ 1
        )

    for j in range(2):
        total = half_own[j, at(z * chunk, chunk), :]
        received = z_recv.at[j, 1:depth]
        remote(received, received, zr_send.at[0], zr_recv.at[j], f, t ^ 1).wait_recv()
        for d in range(1, depth):
            total = total + z_recv[j, d].astype(F32)
        low[j, at(c * half + z * chunk, chunk), :] = total.astype(BF)
        for d in range(1, depth):
            g_copy(j, d).start()
        forward(j, 0).start()

    def block_copy(j, o, side, target):
        piece = basis.at[j, at((2 * o + c) * columns, columns)]
        return remote(
            piece, piece, g_send.at[side, o], g_recv.at[o, j], f, target * 2 + c
        )

    def block_forward(j, o):
        piece = basis.at[j, at((2 * o + c) * columns, columns)]
        return remote(piece, piece, gp_send.at[o], gp_recv.at[o], f, t ^ 1)

    def needed(o):
        return f != (2 * o) // group

    def spread(j, o, side):
        if side == 0:

            @pl.when(z >= 1)
            def _():
                block_copy(j, o, 0, z - 1).start()
        else:

            @pl.when(z <= depth - 2)
            def _():
                block_copy(j, o, 1, z + 1).start()

    @pl.when(needed(z))
    def _():
        for j in range(2):
            for side in range(2):
                spread(j, z, side)

    def arrive(s):
        for side in range(2):
            o = z + s if side == 0 else z - s
            inside = o <= depth - 1 if side == 0 else o >= 0

            @pl.when(inside & needed(o))
            def _(o=o, side=side):
                for j in range(2):
                    block_copy(j, o, side, z).wait_recv()
                    spread(j, o, side)
                    block_forward(j, o).start()

    pltpu.make_async_copy(cot, cot, load_sem.at[5]).wait()

    own = at(f * part, part)

    def project_low(j):
        for d in range(1, depth):
            g_copy(j, d).wait_recv()
            forward(j, d).start()
        received = low.at[j, at((1 - c) * half, half)]
        remote(received, received, pf_send.at[0], pf_recv.at[j], f, t ^ 1).wait_recv()
        product = lax.dot_general(
            low[j], cot[j], (((0,), (0,)), ((), ())), preferred_element_type=F32
        )
        proj[j] = product
        proj_send[j] = product.astype(BF)

    def update_moments(j, summed):
        first = moment_decay * moment[2 * j] + (1.0 - moment_decay) * summed
        second = square_decay * moment[2 * j + 1] + (1.0 - square_decay) * summed * summed
        first_new[j] = first
        second_new[j] = second
        ratio[j, own, :] = (first / jnp.sqrt(second + square_floor)).astype(BF)

    def reduce_copy(j, k):
        near, far = (1, 2) if j == 0 else (2, 1)
        if relay:
            source = proj_mid.at[j] if k == 3 else proj_send.at[j, at((f ^ (near, 3)[k - 1]) * part, part)]
            target = f ^ (far if k == 3 else near)
        else:
            source, target = proj_send.at[j, at((f ^ k) * part, part)], f ^ k
        return remote(
            source, proj_recv.at[j, k], rs_send.at[0], rs_recv.at[j, k - 1], target, t
        )

    def ratio_copy(j, k):
        near, far = (1, 2) if j == 0 else (2, 1)
        if relay:
            piece = ratio.at[j, at((f ^ near) * part, part) if k == 3 else own]
            target = f ^ (near if k == 1 else far)
        else:
            piece, target = ratio.at[j, own], f ^ k
        return remote(piece, piece, ag_send.at[0], ag_recv.at[j, k - 1], target, t)

    for j in range(2):
        project_low(j)
        for k in (2, 1) if relay else range(1, fs):
            reduce_copy(j, k).start()
        if relay:
            share(marks[j], marks[j + 1])

    if relay:
        for j in range(2):
            far = 2 if j == 0 else 1
            reduce_copy(j, 2).wait_recv()
            mid = proj[j, at((f ^ far) * part, part), :] + proj_recv[j, 2].astype(F32)
            proj_mid[j] = mid.astype(BF)
            reduce_copy(j, 3).start()
        share(marks[2], marks[3])
    arrive(1)
    pltpu.make_async_copy(moment, moment, load_sem.at[6]).wait()

    for j in range(2):
        summed = proj[j, own, :]
        for k in (1, 3) if relay else range(1, fs):
            reduce_copy(j, k).wait_recv()
            summed = summed + proj_recv[j, k].astype(F32)
        update_moments(j, summed)
        for k in (1, 2) if relay else range(1, fs):
            ratio_copy(j, k).start()
    if relay:
        share(marks[3], marks[4])
        for j in range(2):
            ratio_copy(j, 1).wait_recv()
            ratio_copy(j, 3).start()
        share(marks[4], marks[5])

    def ratio_wait(j):
        for k in (2, 3) if relay else range(1, fs):
            ratio_copy(j, k).wait_recv()

    if depth > 2:
        arrive(2)

    high = min(rows, 256)
    heads = width // HD
    sums[f] = jnp.zeros(sums.shape[1:], F32)
    for j in range(2):
        ratio_wait(j)

        def add(i, total, j=j):
            update = jnp.dot(
                basis[j, at(f * rows + i * high, high), :], ratio[j], preferred_element_type=F32
            )
            step_ref[j, at(i * high, high), :] = update
            return total + jnp.sum((update * update).reshape(high // 8, 8, width), axis=0)

        squares = lax.fori_loop(0, rows // high, add, jnp.zeros((8, width), F32))
        for h in range(heads):
            total = jnp.sum(squares[:, h * HD : (h + 1) * HD])
            sums[f, j * heads + h : j * heads + h + 1, :] = jnp.broadcast_to(total, (1, HD))

    def sums_copy(m):
        return remote(sums.at[f], sums.at[f], s_send.at[0], s_recv.at[0], f ^ m, t)

    for m in range(1, fs):
        sums_copy(m).start()
    if relay:
        share(marks[5], count)
    for s in range(3, depth):
        arrive(s)
    others = sums.at[0 : fs - 1]
    remote(others, others, s_send.at[0], s_recv.at[0], f ^ 1, t).wait_recv()
    total = sums[0]
    for k in range(1, fs):
        total = total + sums[k]
    factor = 1.0 / jnp.sqrt(total / (fs * rows * HD) + norm_floor)
    for j in range(2):
        for h in range(heads):
            row = factor[j * heads + h : j * heads + h + 1, :]
            scales[j, :, h * HD : (h + 1) * HD] = jnp.broadcast_to(row, (8, HD))

    def finish(j, place, update):
        change = update * (step_rate * scales[j, 0:1, :])
        copy_ref[j, place, :] = (gathered[j, place, :].astype(F32) - change).astype(BF)

    for j in range(2):

        @pl.loop(0, rows // high)
        def _(i, j=j):
            place = at(i * high, high)
            update = step_ref[j, place, :]
            finish(j, at(f * rows + i * high, high), update)
            step = update * scales[j, 0:1, :]
            step_ref[j, place, :] = step
            weight_ref[j, place, :] = master[j, place, :] - step_rate * step

    def both(o, core):
        return basis.at[:, at((2 * o + core) * columns, columns)]

    def partner_block():
        piece = both(z, 1 - c)
        return remote(piece, piece, d_send.at[0], d_recv.at[0], f, t ^ 1)

    @pl.when(role != 0)
    def _():
        partner_block().wait_recv()

    for s in range(1, depth):
        for o, inside in ((z + s, z + s <= depth - 1), (z - s, z - s >= 0)):

            @pl.when(inside & needed(o))
            def _(o=o):
                piece = both(o, 1 - c)
                remote(piece, piece, gp_send.at[o], gp_recv.at[o], f, t ^ 1).wait_recv()

    def finish_rows(j, start, size):
        place = at(start, size)
        update = jnp.dot(basis[j, place, :], ratio[j], preferred_element_type=F32)
        finish(j, place, update)

    large = min(rows, 512)
    pair = 2 * tile

    def finish_block(m, j, wait):
        @pl.loop(0, rows // large)
        def _(i):
            if wait:
                for k in range(large // pair):
                    master_wait(m, j, i * (large // pair) + k)
            finish_rows(j, (f ^ m) * rows + i * large, large)

    if relay:
        finish_block(1, 0, False)
        finish_block(2, 1, False)
        finish_block(1, 1, True)
        finish_block(2, 0, True)

        @pl.loop(0, rows // pair)
        def _(i):
            place = at((f ^ 3) * rows + i * pair, pair)
            for j in range(2):
                update = jnp.dot(basis[j, place, :], ratio[j], preferred_element_type=F32)
                changes[j] = update * (step_rate * scales[j, 0:1, :])
            for j in range(2):
                relay_wait(2 - j, i)
                copy_ref[j, place, :] = (gathered[j, place, :].astype(F32) - changes[j]).astype(BF)
    else:
        for m in range(1, fs):
            for j in range(2):
                finish_block(m, j, True)

    def sent(piece, sem):
        remote(piece, piece, sem, p_recv.at[0], f, t ^ 1).wait_send()

    if relay:
        for k in range(4):

            @pl.when(role == k)
            def _(k=k):
                sent(basis.at[:, 0 : columns if k in (0, 3) else piece_rows], b_send.at[0])
    else:

        @pl.when(role == 0)
        def _():
            for m in range(1, fs):
                sent(basis.at[:, 0:columns], b_send.at[0])

    @pl.when(role != 0)
    def _():
        sent(both(z, c), d_send.at[0])

    sent(half_send, p_send.at[0])
    sent(z_send.at[:, 0 : (depth - 1) * chunk], zr_send.at[0])
    sent(low.at[:, 0 : (depth - 1) * chunk], zg_send.at[0])
    sent(low.at[:, 0 : depth * chunk], pf_send.at[0])
    sent(proj_send.at[:, 0 : (fs - 1) * part], rs_send.at[0])
    sent(ratio.at[:, 0 : (fs - 1) * part], ag_send.at[0])
    sent(others, s_send.at[0])

    for s in range(depth):
        for side in range(2):
            o = z + s if side == 0 else z - s
            there = o <= depth - 1 if side == 0 else o >= 0
            inside = there & (z >= 1) if side == 0 else there & (z <= depth - 2)

            @pl.when(inside & needed(o))
            def _(o=o, side=side):
                sent(both(o, c), g_send.at[side, o])

            if s > 0:

                @pl.when(there & needed(o))
                def _(o=o):
                    sent(both(o, c), gp_send.at[o])

    for m in (1, 2) if relay else range(1, fs):
        piece = gathered.at[:, own_rows]
        remote(piece, piece, m_send.at[m - 1], m_recv.at[m - 1, 0, 0], f ^ m, t).wait_send()
    if relay:
        for m in (1, 2):
            piece = gathered.at[2 - m, own_rows]
            remote(piece, piece, r_send.at[m - 1], r_recv.at[m - 1, 0], f ^ m, t).wait_send()


MARKS = (14, 14, 15, 16, 18, 20)
FIRST = ((8, 8), (5, 2), (2, 5), (4, 4))


def final_kernel(*refs):
    first, second, step, weight, copy = refs[:5]
    outs, sem = refs[5:15], refs[15]
    moves = []
    for j in range(2):
        for k, source in enumerate((step, weight, copy, first, second)):
            moves.append((source.at[j], outs[5 * j + k]))
    moves.sort(key=lambda move: -move[0].size)
    moves = [pltpu.make_async_copy(a, b, sem.at[i]) for i, (a, b) in enumerate(moves)]
    for move in moves:
        move.start()
    for move in moves:
        move.wait()


def body(fs, tp, *args):
    saved_input, query_cot, _, query_master, key_master, query_basis, key_basis = args[:7]
    rows, rank = query_basis.shape
    tokens, columns = saved_input.shape
    width = query_cot.shape[1]
    part = rank // fs
    depth = tp // 2
    count = fs * rows
    half, chunk = tokens // 2, tokens // tp
    pieces = rows // (min(rows, 256) // 2)
    hbm = pl.BlockSpec(memory_space=pltpu.HBM)
    vmem = pl.BlockSpec(memory_space=pltpu.VMEM)
    dma = pltpu.SemaphoreType.DMA
    own = pltpu.VMEM((2, rows, width), F32)
    moment = pltpu.VMEM((2, part, width), F32)
    pairs = [
        *(dma((1,)), dma((2, 2))),
        *(dma((1,)), dma((1,))),
        *(dma((1,)), dma((2,))),
        *(dma((1,)), dma((2,))),
        *(dma((1,)), dma((2, depth - 1))),
        *(dma((1,)), dma((2,))),
        *(dma((2, depth)), dma((depth, 2))),
        *(dma((depth,)), dma((depth,))),
        *(dma((1,)), dma((2, fs - 1))),
        *(dma((1,)), dma((2, fs - 1))),
        *(dma((1,)), dma((1,))),
    ]
    links = 2 if fs == 4 else fs - 1
    pairs += [dma((links,)), dma((links, 2, pieces // 2)), dma((2,)), dma((2, pieces // 2))]
    results = pl.pallas_call(
        functools.partial(exchange_kernel, fs, tp),
        name="exchange",
        out_shape=(moment, moment, own, own, pltpu.VMEM((2, count, width), BF)),
        in_specs=[hbm] * 11,
        out_specs=(vmem,) * 5,
        scratch_shapes=[
            pltpu.VMEM((2, count, rank), BF),
            pltpu.VMEM((2, count, width), BF),
            pltpu.VMEM((tokens, columns), BF),
            pltpu.VMEM((2, tokens, width), BF),
            pltpu.VMEM((2, rows, width), F32),
            pltpu.VMEM((4, part, width), F32),
            pltpu.VMEM((2, half, rank), BF),
            pltpu.VMEM((2, half, rank), BF),
            pltpu.VMEM((2, half, rank), F32),
            pltpu.VMEM((2, half, rank), BF),
            pltpu.VMEM((2, depth, chunk, rank), BF),
            pltpu.VMEM((2, tokens, rank), BF),
            pltpu.VMEM((2, rank, width), F32),
            pltpu.VMEM((2, rank, width), BF),
            pltpu.VMEM((2, fs, part, width), BF),
            pltpu.VMEM((2, part, width), BF),
            pltpu.VMEM((2, rank, width), BF),
            pltpu.VMEM((fs, -(-2 * width // HD // 8) * 8, HD), F32),
            pltpu.VMEM((2, 8, width), F32),
            pltpu.VMEM((2, min(rows, 256), width), F32),
            dma((7,)),
            *pairs,
        ],
        compiler_params=pltpu.CompilerParams(
            collective_id=0, has_side_effects=True, vmem_limit_bytes=40 * 1024 * 1024
        ),
    )(*[pltpu.with_memory_space_constraint(a, pltpu.HBM) for a in args])

    big = jax.ShapeDtypeStruct((rows, width), F32)
    copied = jax.ShapeDtypeStruct((count, width), BF)
    small = jax.ShapeDtypeStruct((part, width), F32)
    return pl.pallas_call(
        final_kernel,
        name="final",
        out_shape=(big, big, copied, small, small) * 2,
        in_specs=[vmem] * 5,
        out_specs=(hbm,) * 10,
        scratch_shapes=[dma((10,))],
        compiler_params=pltpu.CompilerParams(vmem_limit_bytes=20 * 1024 * 1024),
    )(*results)


def solution(mesh):
    split, tall, wide = P("fs", "tp"), P("fs", None), P(None, "tp")
    outs = (split, split, wide, split, split)
    return jax.shard_map(
        functools.partial(body, mesh.shape["fs"], mesh.shape["tp"]),
        mesh=mesh,
        in_specs=(split,) * 5 + (tall, tall) + (split,) * 4,
        out_specs=outs + outs,
        check_vma=False,
    )
```
